512 devices in a mesh: ep: 32 (over z, core), tp: 16 (over y, x).
Axes of the slice: x: 4, y: 4, z: 16, core: 2. Of those that a mesh axis runs over, the one named last changes fastest.
Arguments:
- conv_input: bfloat16 [1024, 65536], P('tp', 'ep'), may hold values from -6 to 6
- out_gate: bfloat16 [1024, 65536], P('tp', 'ep'), may hold values from -6 to 6
- in_gate: bfloat16 [1024, 65536], P('tp', 'ep'), may hold values from -6 to 6
- conv_taps: float32 [3, 1024], replicated, may hold values from -3.5 to 3.5
- mixer_proj: bfloat16 [1024, 2048], P(None, 'tp'), may hold values from -0.1875 to 0.1875
- token_rows: bfloat16 [8192, 2048], P('ep', 'tp'), may hold values from -4000 to 4000
- routes: int32 [8192, 2], P('ep'), may hold values from 0 to 31, as said below
- route_weights: float32 [8192, 2], P('ep'), may hold values from 0.3 to 1
- expert_gate: bfloat16 [32, 2048, 4096], P('ep', None, 'tp'), may hold values from -0.125 to 0.125
- expert_up: bfloat16 [32, 2048, 4096], P('ep', None, 'tp'), may hold values from -0.125 to 0.125
- expert_down: bfloat16 [32, 4096, 2048], P('ep', 'tp'), may hold values from -0.125 to 0.125
Outputs:
- mixed_out: bfloat16 [65536, 2048], P('ep', 'tp')
- expert_out: bfloat16 [8192, 2048], P('ep', 'tp')
The draws below stay inside these ranges and needn't reach their ends.
Inputs may be any that keep to these rules, and one draw needn't show every extreme that they name: `routes`: in each aligned block of 256 rows, no expert is named more than 32 times and one expert, the same in every block, exactly 32 times; the two experts of a row differ.
All inputs are finite; a program needn't handle non-finite values.
Results may differ from the reference program's by a relative error of at most 0.015.
Values may be sent and summed in bfloat16 or wider, within the bound.
No kernel may reach another device: no remote copies, remote signals or barrier semaphores. Data moves between devices by JAX's collectives and lax.ppermute only.
A program may use at most 64 MiB of HBM per device.

```python
import math
import jax
import jax.numpy as jnp
from jax import lax

D = 2048
W = 1024
FF = 4096
KERNEL = 3
ROWS_B = 256
EXPERTS = 32
FF_PART = 256
TOK_A = 65536
TOK_B = 8192
CAP = 32
N_TP = 16


def draw_token_rows(key, part):
    base_key, row_key, col_key = jax.random.split(key, 3)
    ramp = jnp.arange(D, dtype=jnp.float32) / D
    base = jnp.clip(jax.random.normal(base_key, (TOK_B, D), jnp.float32), -6.0, 6.0)
    row_scales = jnp.exp(jax.random.uniform(row_key, (TOK_B, 1), jnp.float32, 0.0, math.log(10.0)))
    col_scales = jnp.exp(math.log(10.0) * ramp) * jnp.exp(jax.random.uniform(col_key, (D,), jnp.float32, -0.4, 0.4))
    return (base * row_scales * col_scales[None, :]).astype(jnp.bfloat16)


def draw_routes(key, part):
    blocks = TOK_B // ROWS_B
    capacity = 4 * ROWS_B // EXPERTS
    spare = 2 * ROWS_B - capacity
    hottest = jax.random.randint(jax.random.fold_in(key, 7), (), 0, EXPERTS).astype(jnp.int32)
    ladder = jnp.arange(EXPERTS - 1, dtype=jnp.int32)
    weight_cum = (ladder + 1) * (ladder + 2) // 2
    weight_total = (EXPERTS - 1) * EXPERTS // 2
    run_ends = capacity + spare * weight_cum // weight_total
    position = jnp.arange(2 * ROWS_B, dtype=jnp.int32)
    which_run = jnp.sum((position[:, None] >= run_ends[None, :]).astype(jnp.int32), axis=1)
    which_run = jnp.minimum(which_run, EXPERTS - 2)

    def one_block(block_index):
        block_key = jax.random.fold_in(key, block_index + 11)
        order = jax.random.permutation(jax.random.fold_in(block_key, 1), EXPERTS - 1).astype(jnp.int32)
        others = (hottest + 1 + order) % EXPERTS
        listing = jnp.where(position < capacity, hottest, others[which_run])
        pairs = jnp.stack([listing[:ROWS_B], listing[ROWS_B:]], axis=1)
        shuffle = jax.random.permutation(jax.random.fold_in(block_key, 2), ROWS_B)
        return pairs[shuffle]
    table = jax.vmap(one_block)(jnp.arange(blocks, dtype=jnp.int32))
    return table.reshape(TOK_B, 2).astype(jnp.int32)


def spiked(drawn, rng, source, target, shards_of, factor):
    owner, partner = [(jnp.arange(drawn.shape[axis_at]) // (drawn.shape[axis_at] // shards_of)).reshape([-1 if axis == axis_at else 1 for axis in range(drawn.ndim)]) for axis_at in (source, target)]
    chosen = jax.random.permutation(rng, shards_of)[partner]
    strong = (owner == chosen) | (owner == (partner + shards_of // 2) % shards_of)
    return jnp.where(strong, factor * drawn, drawn)


def levels(rng, dims, shards, least, largest):
    def one(dim, blocks):
        heights = jax.random.uniform(jax.random.fold_in(jax.random.fold_in(rng, 6), dim), (blocks,), jnp.float32, least / len(shards), largest / len(shards))
        return jnp.repeat(jnp.exp(heights), dims[dim] // blocks).reshape((-1,) + (1,) * (len(dims) - dim - 1))

    factor_of = one(*shards[0])
    for cut in shards[1:]:
        factor_of = factor_of * one(*cut)
    return factor_of


def bell_draw(key, extent, scale, limit, pieces=(), kind=jnp.bfloat16):
    result = jax.random.normal(key, extent, jnp.float32) * scale
    if len(pieces) > 0:
        result = levels(key, extent, pieces, -0.22, 0.18) * result
    return jnp.clip(result, min=-limit, max=limit).astype(kind)


def noise_with(rng, shape, width, bound, cuts, heavy, held_as=jnp.bfloat16):
    drawn = width * jax.random.normal(rng, shape, jnp.float32)
    if cuts:
        drawn = drawn * levels(rng, shape, cuts, -0.22, 0.18)
    return jnp.clip(spiked(drawn, jax.random.fold_in(rng, 3), *heavy), -bound, bound).astype(held_as)


def setup_inputs(seed: int = 0) -> dict:
    seeds = jax.random.split(jax.random.key(seed), 12)
    return {
        "conv_input": bell_draw(seeds[0], (W, TOK_A), 1.0, 6.0, ((0, 16), (1, 32))),
        "out_gate": bell_draw(seeds[1], (W, TOK_A), 1.0, 6.0, ((0, 16), (1, 32))),
        "in_gate": bell_draw(seeds[2], (W, TOK_A), 1.0, 6.0, ((0, 16), (1, 32))),
        "conv_taps": bell_draw(seeds[3], (KERNEL, W), 0.6, 3.5, (), jnp.float32),
        "mixer_proj": bell_draw(seeds[4], (W, D), W ** -0.5, 0.1875, ((1, 16),)),
        "token_rows": draw_token_rows(jax.random.fold_in(seeds[11], 71), 0),
        "routes": draw_routes(jax.random.fold_in(seeds[11], 71), 0),
        "route_weights": jnp.clip(0.3 + 0.7 * jax.random.uniform(seeds[7], (TOK_B, 2), jnp.float32) ** levels(seeds[7], (TOK_B, 2), ((0, 32),), -0.2, 0.2), 0.3, 1.0),
        "expert_gate": bell_draw(seeds[8], (EXPERTS, D, FF), D ** -0.5, 0.125, ((0, 32), (2, 16))),
        "expert_up": bell_draw(seeds[9], (EXPERTS, D, FF), D ** -0.5, 0.125, ((0, 32), (2, 16))),
        "expert_down": noise_with(seeds[10], (EXPERTS, FF, D), FF ** -0.5, 0.125, ((0, 32), (1, 16)), (1, 2, 16, 2.0)),
    }


EPSILON = 1e-06

def slot_places(route_ids, capacity, experts):
    flat_ids = route_ids.reshape(-1).astype(jnp.int32)
    hit_table = (flat_ids[:, None] == jnp.arange(experts, dtype=jnp.int32)[None, :]).astype(jnp.int32)
    earlier = jnp.cumsum(hit_table, axis=0) - hit_table
    slot_rank = lax.optimization_barrier(jnp.sum(earlier * hit_table, axis=1))
    return (flat_ids * capacity + slot_rank).astype(jnp.int32)

def mixer(conv_input, out_gate, in_gate, conv_taps, mixer_proj):
    z_rows = (conv_input.astype(jnp.float32) * in_gate.astype(jnp.float32)).astype(jnp.bfloat16)
    length = z_rows.shape[1]
    padded = jnp.pad(z_rows.astype(jnp.float32), ((0, 0), (KERNEL - 1, 0)))
    conv_sum = jnp.zeros(z_rows.shape, jnp.float32)
    for lag_index in range(KERNEL):
        begin = KERNEL - 1 - lag_index
        conv_sum = conv_sum + conv_taps[lag_index][:, None] * padded[:, begin:begin + length]
    gated = (out_gate.astype(jnp.float32) * conv_sum).astype(jnp.bfloat16)
    return jnp.dot(gated.T, mixer_proj, preferred_element_type=jnp.float32).astype(jnp.bfloat16)

def expert_block(inputs):
    rows_in, gate_weight, up_weight, down_weight = inputs
    values = rows_in.astype(jnp.float32)
    row_scale = lax.rsqrt(lax.optimization_barrier(jnp.mean(values * values, axis=1, keepdims=True)) + EPSILON)
    gate_sum = row_scale * jnp.dot(rows_in, gate_weight, preferred_element_type=jnp.float32)
    up_sum = row_scale * jnp.dot(rows_in, up_weight, preferred_element_type=jnp.float32)
    hidden = (jax.nn.silu(gate_sum) * up_sum).astype(jnp.bfloat16)
    split_hidden = hidden.reshape(hidden.shape[0], N_TP, FF_PART).astype(jnp.float32)
    split_down = down_weight.reshape(N_TP, FF_PART, D).astype(jnp.float32)
    partial_value = jnp.einsum('snf,nfd->nsd', split_hidden, split_down).astype(jnp.bfloat16)
    return lax.optimization_barrier(jnp.sum(partial_value.astype(jnp.float32), axis=0)).astype(jnp.bfloat16)

def reference(conv_input, out_gate, in_gate, conv_taps, mixer_proj, token_rows, routes, route_weights, expert_gate, expert_up, expert_down):
    mixed_out = mixer(conv_input, out_gate, in_gate, conv_taps, mixer_proj)
    blocks = TOK_B // ROWS_B
    route_blocks = routes.reshape(blocks, ROWS_B, 2)

    def block_places(route_ids):
        return slot_places(route_ids, CAP, EXPERTS)
    places = jax.vmap(block_places)(route_blocks)
    sources = jnp.arange(2 * ROWS_B, dtype=jnp.int32) // 2

    def fill(rows_in, place_list):
        return jnp.zeros((EXPERTS * CAP, D), jnp.bfloat16).at[place_list].set(rows_in[sources])
    buffers = jax.vmap(fill)(token_rows.reshape(blocks, ROWS_B, D), places)
    by_expert = buffers.reshape(blocks, EXPERTS, CAP, D).transpose(1, 0, 2, 3).reshape(EXPERTS, blocks * CAP, D)
    results = lax.map(expert_block, (by_expert, expert_gate, expert_up, expert_down))
    home = results.reshape(EXPERTS, blocks, CAP, D).transpose(1, 0, 2, 3).reshape(blocks, EXPERTS * CAP, D)

    def pick(rows_in, place_list):
        return rows_in[place_list]
    picked = jax.vmap(pick)(home, places).astype(jnp.float32).reshape(blocks, ROWS_B, 2, D)
    weights = route_weights.reshape(blocks, ROWS_B, 2, 1)
    expert_out = lax.optimization_barrier(jnp.sum(picked * weights, axis=2)).reshape(TOK_B, D).astype(jnp.bfloat16)
    return (mixed_out, expert_out)
```

```python
import jax
import jax.numpy as jnp
from jax import lax
from jax.experimental import pallas as pl
from jax.experimental.pallas import tpu as pltpu
from jax.sharding import Mesh
from jax.sharding import PartitionSpec as P

KERNEL = 3
EPSILON = 1e-06
BF = jnp.bfloat16
F32 = jnp.float32


def expert_kernel(x_ref, gate_ref, up_ref, down_ref, out_ref):
    parts = x_ref.shape[0]
    cols = x_ref.shape[2]
    x = jnp.concatenate([x_ref[j] for j in range(parts)], axis=1)
    values = x.astype(F32)
    squares = jnp.sum(values * values, axis=1, keepdims=True)
    scale = lax.rsqrt(squares / (parts * cols) + EPSILON)
    gate = scale * jnp.dot(x, gate_ref[...], preferred_element_type=F32)
    up = scale * jnp.dot(x, up_ref[...], preferred_element_type=F32)
    hidden = (jax.nn.silu(gate) * up).astype(BF)
    part = jnp.dot(hidden, down_ref[...], preferred_element_type=F32).astype(BF)
    for j in range(parts):
        out_ref[j] = part[:, j * cols : (j + 1) * cols]


def expert_part(x, gate_weight, up_weight, down_weight, tile):
    parts, rows, cols = x.shape
    whole = lambda w: pl.BlockSpec(w.shape, lambda i: (0, 0))
    return pl.pallas_call(
        expert_kernel,
        grid=(rows // tile,),
        in_specs=[
            pl.BlockSpec((parts, tile, cols), lambda i: (0, i, 0)),
            whole(gate_weight),
            whole(up_weight),
            whole(down_weight),
        ],
        out_specs=pl.BlockSpec((parts, tile, cols), lambda i: (0, i, 0)),
        out_shape=jax.ShapeDtypeStruct(x.shape, BF),
        compiler_params=pltpu.CompilerParams(vmem_limit_bytes=40 * 1024 * 1024),
        cost_estimate=pl.CostEstimate(
            flops=6 * rows * parts * cols * gate_weight.shape[1],
            bytes_accessed=2 * 2 * rows * parts * cols + 6 * gate_weight.size,
            transcendentals=rows * gate_weight.shape[1],
        ),
    )(x, gate_weight, up_weight, down_weight)


def sum_parts(arrived):
    return arrived.astype(F32).sum(axis=0).astype(BF)


def body(
    conv_input,
    out_gate,
    in_gate,
    conv_taps,
    mixer_proj,
    token_rows,
    routes,
    route_weights,
    expert_gate,
    expert_up,
    expert_down,
):
    depth = lax.axis_size("z")
    experts = 2 * depth
    tp = lax.axis_size("tp")
    core = lax.axis_index("c")
    rows_b, cols_part = token_rows.shape
    capacity = 4 * rows_b // experts
    slot_total = experts * capacity
    half = slot_total // 2

    expert_ids = jnp.arange(experts, dtype=jnp.int32)[None, :]
    hit0 = routes[:, 0:1] == expert_ids
    hit1 = routes[:, 1:2] == expert_ids
    hits = (hit0 | hit1).astype(BF)
    order = jnp.arange(rows_b, dtype=jnp.int32)
    earlier_rows = (order[None, :] < order[:, None]).astype(BF)
    earlier = jnp.dot(earlier_rows, hits, preferred_element_type=F32).astype(jnp.int32)
    places = []
    for k, hit in enumerate((hit0, hit1)):
        slot = jnp.sum(jnp.where(hit, earlier, 0), axis=1)
        places.append((routes[:, k] ^ core) * capacity + slot)
    slot_ids = jnp.arange(slot_total, dtype=jnp.int32)[None, :]
    pick0 = places[0][:, None] == slot_ids
    pick1 = places[1][:, None] == slot_ids
    pick_any = (pick0 | pick1).astype(BF)
    outgoing = lax.dot_general(
        pick_any, token_rows, (((0,), (0,)), ((), ())), preferred_element_type=F32
    ).astype(BF)

    length = conv_input.shape[1]
    width_part = conv_input.shape[0]
    offset = lax.axis_index("tp") * width_part
    local_taps = lax.dynamic_slice_in_dim(conv_taps, offset, width_part, 1)
    rim_from = length - (KERNEL - 1)
    rim = (
        conv_input[:, rim_from:].astype(F32) * in_gate[:, rim_from:].astype(F32)
    ).astype(BF)
    pairs = [(i, i + 1) for i in range(experts - 1)]
    rim = lax.ppermute(rim, ("z", "c"), pairs)
    z_rows = (conv_input.astype(F32) * in_gate.astype(F32)).astype(BF)
    longer = jnp.concatenate([rim, z_rows], axis=1).astype(F32)
    conv_sum = jnp.zeros(z_rows.shape, F32)
    for lag in range(KERNEL):
        begin = KERNEL - 1 - lag
        conv_sum = conv_sum + local_taps[lag][:, None] * longer[:, begin : begin + length]
    gated = (out_gate.astype(F32) * conv_sum).astype(BF)
    first = gated[:, : length // 2]
    y_first = lax.all_gather(first, "tp", axis=0, tiled=True)

    swap = [(0, 1), (1, 0)]
    arrived = lax.all_to_all(
        outgoing.reshape(depth, 2, capacity, cols_part), "z", 0, 0, tiled=True
    )
    arrived, gated = lax.optimization_barrier((arrived, gated))
    rows_own = arrived[:, 0].reshape(half, cols_part)
    rows_other = lax.ppermute(arrived[:, 1].reshape(half, cols_part), "c", swap)

    x_own = lax.all_gather(rows_own, "tp", axis=0, tiled=False)
    x_other = lax.all_to_all(
        jnp.broadcast_to(rows_other[None], (tp, half, cols_part)), "tp", 0, 0, tiled=True
    )
    second, x_other = lax.optimization_barrier((gated[:, length // 2 :], x_other))
    y_second = lax.all_gather(second, "tp", axis=0, tiled=True)

    weights = (expert_gate[0], expert_up[0], expert_down[0])
    tile = half // 2
    part_other = expert_part(x_other, *weights, tile)
    sums_other = lax.all_to_all(part_other, "tp", 0, 0, tiled=True)
    part_own = expert_part(x_own, *weights, tile)
    part_own, sums_other = lax.optimization_barrier((part_own, sums_other))
    sums_own = lax.all_to_all(part_own, "tp", 0, 0, tiled=True)
    back_other = lax.ppermute(sum_parts(sums_other), "c", swap)
    back_own = sum_parts(sums_own)
    back = jnp.stack(
        [
            back_own.reshape(depth, capacity, cols_part),
            back_other.reshape(depth, capacity, cols_part),
        ],
        axis=1,
    )
    returned = lax.all_to_all(back, "z", 0, 0, tiled=True).reshape(slot_total, cols_part)
    picked0 = jnp.dot(pick0.astype(BF), returned, preferred_element_type=F32)
    picked1 = jnp.dot(pick1.astype(BF), returned, preferred_element_type=F32)
    expert_out = (
        picked0 * route_weights[:, 0:1] + picked1 * route_weights[:, 1:2]
    ).astype(BF)

    mixed = [
        lax.dot_general(
            y, mixer_proj, (((0,), (0,)), ((), ())), preferred_element_type=F32
        ).astype(BF)
        for y in (y_first, y_second)
    ]
    mixed_out = jnp.concatenate(mixed, axis=0)
    return (mixed_out, expert_out)


def solution(mesh):
    ep, tp = mesh.devices.shape
    fine = Mesh(mesh.devices.reshape(ep // 2, 2, tp), ("z", "c", "tp"))
    both = ("z", "c")
    return jax.shard_map(
        body,
        mesh=fine,
        in_specs=(
            P("tp", both),
            P("tp", both),
            P("tp", both),
            P(),
            P(None, "tp"),
            P(both, "tp"),
            P(both, None),
            P(both, None),
            P(both, None, "tp"),
            P(both, None, "tp"),
            P(both, "tp", None),
        ),
        out_specs=(P(both, "tp"), P(both, "tp")),
        check_vma=False,
    )
```

```python
import jax
import jax.numpy as jnp
from jax import lax
from jax.experimental import pallas as pl
from jax.experimental.pallas import tpu as pltpu
from jax.sharding import Mesh
from jax.sharding import PartitionSpec as P

KERNEL = 3
EPSILON = 1e-06
BF = jnp.bfloat16
F32 = jnp.float32


def expert_kernel(core_ref, x_ref, gate_ref, up_ref, down_ref, out_ref):
    parts = x_ref.shape[0]
    cols = x_ref.shape[2]
    side = 4
    core = core_ref[0]
    natural = [j for j in range(parts)]
    turned = [(j % side) * side + j // side for j in range(parts)]
    load = [jnp.where(core == 0, natural[j], turned[j]) for j in range(parts)]
    store = [jnp.where(core == 0, turned[j], natural[j]) for j in range(parts)]
    x = jnp.concatenate([x_ref[load[j]] for j in range(parts)], axis=1)
    values = x.astype(F32)
    squares = jnp.sum(values * values, axis=1, keepdims=True)
    scale = lax.rsqrt(squares / (parts * cols) + EPSILON)
    gate = scale * jnp.dot(x, gate_ref[...], preferred_element_type=F32)
    up = scale * jnp.dot(x, up_ref[...], preferred_element_type=F32)
    hidden = (jax.nn.silu(gate) * up).astype(BF)
    part = jnp.dot(hidden, down_ref[...], preferred_element_type=F32).astype(BF)
    for j in range(parts):
        out_ref[store[j]] = part[:, j * cols : (j + 1) * cols]


def expert_part(core, x, gate_weight, up_weight, down_weight, tile):
    parts, rows, cols = x.shape
    whole = lambda w: pl.BlockSpec(w.shape, lambda i, c: (0, 0))
    return pl.pallas_call(
        expert_kernel,
        grid_spec=pltpu.PrefetchScalarGridSpec(
            num_scalar_prefetch=1,
            grid=(rows // tile,),
            in_specs=[
                pl.BlockSpec((parts, tile, cols), lambda i, c: (0, i, 0)),
                whole(gate_weight),
                whole(up_weight),
                whole(down_weight),
            ],
            out_specs=pl.BlockSpec((parts, tile, cols), lambda i, c: (0, i, 0)),
        ),
        out_shape=jax.ShapeDtypeStruct(x.shape, BF),
        compiler_params=pltpu.CompilerParams(vmem_limit_bytes=28 * 1024 * 1024),
        cost_estimate=pl.CostEstimate(
            flops=6 * rows * parts * cols * gate_weight.shape[1],
            bytes_accessed=2 * 2 * rows * parts * cols + 6 * gate_weight.size,
            transcendentals=rows * gate_weight.shape[1],
        ),
    )(core.reshape(1), x, gate_weight, up_weight, down_weight)


def sum_parts(arrived):
    return arrived.astype(F32).sum(axis=0).astype(BF)


def body(
    conv_input,
    out_gate,
    in_gate,
    conv_taps,
    mixer_proj,
    token_rows,
    routes,
    route_weights,
    expert_gate,
    expert_up,
    expert_down,
):
    depth = lax.axis_size("z")
    experts = 2 * depth
    tp = lax.axis_size("tp")
    core = lax.axis_index("c")
    rows_b, cols_part = token_rows.shape
    capacity = 4 * rows_b // experts
    slot_total = experts * capacity
    half = slot_total // 2

    expert_ids = jnp.arange(experts, dtype=jnp.int32)[None, :]
    hit0 = routes[:, 0:1] == expert_ids
    hit1 = routes[:, 1:2] == expert_ids
    hits = (hit0 | hit1).astype(BF)
    order = jnp.arange(rows_b, dtype=jnp.int32)
    earlier_rows = (order[None, :] < order[:, None]).astype(BF)
    earlier = jnp.dot(earlier_rows, hits, preferred_element_type=F32).astype(jnp.int32)
    places = []
    for k, hit in enumerate((hit0, hit1)):
        slot = jnp.sum(jnp.where(hit, earlier, 0), axis=1)
        places.append((routes[:, k] ^ core) * capacity + slot)
    slot_ids = jnp.arange(slot_total, dtype=jnp.int32)[None, :]
    pick0 = places[0][:, None] == slot_ids
    pick1 = places[1][:, None] == slot_ids
    pick_any = (pick0 | pick1).astype(BF)
    outgoing = lax.dot_general(
        pick_any, token_rows, (((0,), (0,)), ((), ())), preferred_element_type=F32
    ).astype(BF)

    outgoing, conv_input, in_gate = lax.optimization_barrier((outgoing, conv_input, in_gate))
    arrived = lax.all_to_all(
        outgoing.reshape(depth, 2, capacity, cols_part), "z", 0, 0, tiled=True
    )

    length = conv_input.shape[1]
    width_part = conv_input.shape[0]
    offset = lax.axis_index("tp") * width_part
    local_taps = lax.dynamic_slice_in_dim(conv_taps, offset, width_part, 1)
    z_rows = (conv_input.astype(F32) * in_gate.astype(F32)).astype(BF)
    pairs = [(i, i + 1) for i in range(experts - 1)]
    rim = lax.ppermute(z_rows[:, length - (KERNEL - 1) :], ("z", "c"), pairs)
    longer = jnp.concatenate([rim, z_rows], axis=1).astype(F32)
    conv_sum = jnp.zeros(z_rows.shape, F32)
    for lag in range(KERNEL):
        begin = KERNEL - 1 - lag
        conv_sum = conv_sum + local_taps[lag][:, None] * longer[:, begin : begin + length]
    gated = (out_gate.astype(F32) * conv_sum).astype(BF)
    y = lax.all_gather(gated, "tp", axis=0, tiled=True)
    arrived, gated = lax.optimization_barrier((arrived, gated))

    side = 4
    swap = [(0, 1), (1, 0)]
    place = lambda c, y, x: (c * side + y) * side + x
    span = range(side)
    along_x = lambda c: [[place(c, y, x) for x in span] for y in span]
    along_y = lambda c: [[place(c, y, x) for y in span] for x in span]
    early = along_x(0) + along_y(1)
    late = along_y(0) + along_x(1)

    def exchange(value, groups):
        return lax.all_to_all(
            value, ("c", "tp"), 0, 0, axis_index_groups=groups, tiled=True
        )

    def spread(value, groups):
        return exchange(jnp.broadcast_to(value[None], (side,) + value.shape), groups)

    rows_own = arrived[:, 0].reshape(half, cols_part)
    rows_other = lax.ppermute(arrived[:, 1].reshape(half, cols_part), "c", swap)
    rows = jnp.concatenate([rows_own, rows_other], axis=0)
    x = spread(spread(rows, early), late).reshape(tp, slot_total, cols_part)
    weights = (expert_gate[0], expert_up[0], expert_down[0])
    part = expert_part(core, x, *weights, rows_b)
    part = part.reshape(side, side, slot_total, cols_part)
    expert_rows = sum_parts(exchange(sum_parts(exchange(part, early)), late))
    back_own = expert_rows[:half]
    back_other = lax.ppermute(expert_rows[half:], "c", swap)
    back = jnp.stack(
        [
            back_own.reshape(depth, capacity, cols_part),
            back_other.reshape(depth, capacity, cols_part),
        ],
        axis=1,
    )
    mixed_out = lax.dot_general(
        y, mixer_proj, (((0,), (0,)), ((), ())), preferred_element_type=F32
    ).astype(BF)
    returned = lax.all_to_all(back, "z", 0, 0, tiled=True)
    returned, mixed_out = lax.optimization_barrier((returned, mixed_out))
    returned = returned.reshape(slot_total, cols_part)
    picked0 = jnp.dot(pick0.astype(BF), returned, preferred_element_type=F32)
    picked1 = jnp.dot(pick1.astype(BF), returned, preferred_element_type=F32)
    expert_out = (
        picked0 * route_weights[:, 0:1] + picked1 * route_weights[:, 1:2]
    ).astype(BF)

    return (mixed_out, expert_out)


def solution(mesh):
    ep, tp = mesh.devices.shape
    fine = Mesh(mesh.devices.reshape(ep // 2, 2, tp), ("z", "c", "tp"))
    both = ("z", "c")
    return jax.shard_map(
        body,
        mesh=fine,
        in_specs=(
            P("tp", both),
            P("tp", both),
            P("tp", both),
            P(),
            P(None, "tp"),
            P(both, "tp"),
            P(both, None),
            P(both, None),
            P(both, None, "tp"),
            P(both, None, "tp"),
            P(both, "tp", None),
        ),
        out_specs=(P(both, "tp"), P(both, "tp")),
        check_vma=False,
    )
```

```python
import jax
import jax.numpy as jnp
from jax import lax
from jax.experimental import pallas as pl
from jax.experimental.pallas import tpu as pltpu
from jax.sharding import Mesh
from jax.sharding import PartitionSpec as P

KERNEL = 3
EPSILON = 1e-06
BF = jnp.bfloat16
F32 = jnp.float32


def expert_kernel(me_ref, x_ref, gate_ref, up_ref, down_ref, out_ref):
    parts = x_ref.shape[0]
    cols = x_ref.shape[2]
    side = 4
    core = me_ref[0] // parts
    natural = [j for j in range(parts)]
    turned = [(j % side) * side + j // side for j in range(parts)]
    load = [jnp.where(core == 0, natural[j], turned[j]) for j in range(parts)]
    store = [jnp.where(core == 0, turned[j], natural[j]) for j in range(parts)]
    x = jnp.concatenate([x_ref[load[j]] for j in range(parts)], axis=1)
    values = x.astype(F32)
    squares = jnp.sum(values * values, axis=1, keepdims=True)
    scale = lax.rsqrt(squares / (parts * cols) + EPSILON)
    gate = scale * jnp.dot(x, gate_ref[...], preferred_element_type=F32)
    up = scale * jnp.dot(x, up_ref[...], preferred_element_type=F32)
    hidden = (jax.nn.silu(gate) * up).astype(BF)
    part = jnp.dot(hidden, down_ref[...], preferred_element_type=F32).astype(BF)
    for j in range(parts):
        out_ref[store[j]] = part[:, j * cols : (j + 1) * cols]


def expert_part(me, x, gate_weight, up_weight, down_weight, tile):
    parts, rows, cols = x.shape
    whole = lambda w: pl.BlockSpec(w.shape, lambda i, c: (0, 0))
    return pl.pallas_call(
        expert_kernel,
        grid_spec=pltpu.PrefetchScalarGridSpec(
            num_scalar_prefetch=1,
            grid=(rows // tile,),
            in_specs=[
                pl.BlockSpec((parts, tile, cols), lambda i, c: (0, i, 0)),
                whole(gate_weight),
                whole(up_weight),
                whole(down_weight),
            ],
            out_specs=pl.BlockSpec((parts, tile, cols), lambda i, c: (0, i, 0)),
        ),
        out_shape=jax.ShapeDtypeStruct(x.shape, BF),
        compiler_params=pltpu.CompilerParams(vmem_limit_bytes=28 * 1024 * 1024),
        cost_estimate=pl.CostEstimate(
            flops=6 * rows * parts * cols * gate_weight.shape[1],
            bytes_accessed=2 * 2 * rows * parts * cols + 6 * gate_weight.size,
            transcendentals=rows * gate_weight.shape[1],
        ),
    )(me.reshape(1), x, gate_weight, up_weight, down_weight)


def mixer_kernel(me_ref, y0_ref, y1_ref, y2a_ref, y2b_ref, y3_ref, proj_ref, out_ref):
    blocks = proj_ref.shape[0]
    side = 4
    core = me_ref[0] // blocks
    row = (me_ref[0] % blocks) // side
    col = me_ref[0] % side
    weights = []
    for far in range(side):
        for near in range(side):
            down = jnp.where(core == 0, far, near)
            right = jnp.where(core == 0, near, far)
            at = ((row + down) % side) * side + (col + right) % side
            weights.append(proj_ref[at])
    proj = jnp.concatenate(weights, axis=0)
    pieces = [
        ref[i]
        for ref in (y0_ref, y1_ref, y2a_ref, y2b_ref, y3_ref)
        for i in range(ref.shape[0])
    ]
    y = jnp.concatenate(pieces, axis=0)
    flat = lax.dot_general(
        proj, y, (((0,), (0,)), ((), ())), preferred_element_type=F32
    )
    out_ref[...] = jnp.transpose(flat).astype(BF)


def mixer_product(me, pieces, proj, tile):
    length = pieces[0].shape[2]
    blocks, width, cols = proj.shape
    return pl.pallas_call(
        mixer_kernel,
        grid_spec=pltpu.PrefetchScalarGridSpec(
            num_scalar_prefetch=1,
            grid=(length // tile,),
            in_specs=[
                pl.BlockSpec(p.shape[:2] + (tile,), lambda i, c: (0, 0, i)) for p in pieces
            ]
            + [pl.BlockSpec(proj.shape, lambda i, c: (0, 0, 0))],
            out_specs=pl.BlockSpec((tile, cols), lambda i, c: (i, 0)),
        ),
        out_shape=jax.ShapeDtypeStruct((length, cols), BF),
        compiler_params=pltpu.CompilerParams(vmem_limit_bytes=20 * 1024 * 1024),
        cost_estimate=pl.CostEstimate(
            flops=2 * length * blocks * width * cols,
            bytes_accessed=2 * length * (blocks * width + cols) + 2 * proj.size,
            transcendentals=0,
        ),
    )(me.reshape(1), *pieces, proj)


def sum_parts(arrived):
    return arrived.astype(F32).sum(axis=0).astype(BF)


def layer(
    conv_input,
    out_gate,
    in_gate,
    conv_taps,
    mixer_proj,
    token_rows,
    routes,
    route_weights,
    expert_gate,
    expert_up,
    expert_down,
):
    depth = lax.axis_size("z")
    experts = 2 * depth
    tp = lax.axis_size("tp")
    core = lax.axis_index("c")
    me = lax.axis_index(("c", "tp"))
    rows_b, cols_part = token_rows.shape
    capacity = 4 * rows_b // experts
    slot_total = experts * capacity
    half = slot_total // 2

    expert_ids = jnp.arange(experts, dtype=jnp.int32)[None, :]
    hit0 = routes[:, 0:1] == expert_ids
    hit1 = routes[:, 1:2] == expert_ids
    hits = (hit0 | hit1).astype(BF)
    order = jnp.arange(rows_b, dtype=jnp.int32)
    earlier_rows = (order[None, :] < order[:, None]).astype(BF)
    earlier = jnp.dot(earlier_rows, hits, preferred_element_type=F32).astype(jnp.int32)
    places = []
    for k, hit in enumerate((hit0, hit1)):
        slot = jnp.sum(jnp.where(hit, earlier, 0), axis=1)
        places.append((routes[:, k] ^ core) * capacity + slot)
    slot_ids = jnp.arange(slot_total, dtype=jnp.int32)[None, :]
    pick0 = places[0][:, None] == slot_ids
    pick1 = places[1][:, None] == slot_ids
    pick_any = (pick0 | pick1).astype(BF)
    outgoing = lax.dot_general(
        pick_any, token_rows, (((0,), (0,)), ((), ())), preferred_element_type=F32
    ).astype(BF)

    outgoing, conv_input, in_gate = lax.optimization_barrier((outgoing, conv_input, in_gate))
    arrived = lax.all_to_all(
        outgoing.reshape(depth, 2, capacity, cols_part), "z", 0, 0, tiled=True
    )

    length = conv_input.shape[1]
    width_part = conv_input.shape[0]
    offset = lax.axis_index("tp") * width_part
    local_taps = lax.dynamic_slice_in_dim(conv_taps, offset, width_part, 1)
    z_rows = (conv_input.astype(F32) * in_gate.astype(F32)).astype(BF)
    pairs = [(i, i + 1) for i in range(experts - 1)]
    rim = lax.ppermute(z_rows[:, length - (KERNEL - 1) :], ("z", "c"), pairs)
    longer = jnp.concatenate([rim, z_rows], axis=1).astype(F32)
    conv_sum = jnp.zeros(z_rows.shape, F32)
    for lag in range(KERNEL):
        begin = KERNEL - 1 - lag
        conv_sum = conv_sum + local_taps[lag][:, None] * longer[:, begin : begin + length]
    gated = (out_gate.astype(F32) * conv_sum).astype(BF)
    side = 4
    swap = [(0, 1), (1, 0)]
    place = lambda c, y, x: (c * side + y) * side + x
    span = range(side)
    along_x = lambda c: [[place(c, y, x) for x in span] for y in span]
    along_y = lambda c: [[place(c, y, x) for y in span] for x in span]
    early = along_x(0) + along_y(1)
    late = along_y(0) + along_x(1)

    def step(value, by, phase):
        pairs = []
        for c in range(2):
            for y in span:
                for x in span:
                    if (c == 0) == (phase == 0):
                        to = place(c, y, (x + by) % side)
                    else:
                        to = place(c, (y + by) % side, x)
                    pairs.append((place(c, y, x), to))
        return lax.ppermute(value, ("c", "tp"), pairs)

    gated = gated.reshape(2, width_part // 2, length)
    before = step(gated, 1, 0)
    after = step(gated, -1, 0)
    far_a = step(before[:1], 1, 0)
    far_b = step(after[1:], -1, 0)
    line = jnp.concatenate([gated, after, far_a, far_b, before], axis=0)
    arrived, line = lax.optimization_barrier((arrived, line))

    def exchange(value, groups):
        return lax.all_to_all(
            value, ("c", "tp"), 0, 0, axis_index_groups=groups, tiled=True
        )

    def spread(value, groups):
        return exchange(jnp.broadcast_to(value[None], (side,) + value.shape), groups)

    rows_own = arrived[:, 0].reshape(half, cols_part)
    rows_other = lax.ppermute(arrived[:, 1].reshape(half, cols_part), "c", swap)
    rows = jnp.concatenate([rows_own, rows_other], axis=0)
    x = spread(spread(rows, early), late).reshape(tp, slot_total, cols_part)
    weights = (expert_gate[0], expert_up[0], expert_down[0])
    part = expert_part(me, x, *weights, rows_b)
    part = part.reshape(side, side, slot_total, cols_part)
    half_sums = sum_parts(exchange(part, early))
    half_sums, line = lax.optimization_barrier((half_sums, line))
    line_before = step(line, 1, 1)
    line_after = step(line, -1, 1)
    expert_rows = exchange(half_sums, late)
    expert_rows = sum_parts(expert_rows)
    back_own = expert_rows[:half]
    back_other = lax.ppermute(expert_rows[half:], "c", swap)
    back = jnp.stack(
        [
            back_own.reshape(depth, capacity, cols_part),
            back_other.reshape(depth, capacity, cols_part),
        ],
        axis=1,
    )
    back, near_a, near_b = lax.optimization_barrier((back, line_before[:4], line_after[4:]))
    line_far_a = step(near_a, 1, 1)
    line_far_b = step(near_b, -1, 1)
    returned = lax.all_to_all(back, "z", 0, 0, tiled=True)
    mixed_out = mixer_product(
        me,
        (line, line_after, line_far_a, line_far_b, line_before),
        mixer_proj.reshape(tp, width_part, cols_part),
        length // 4,
    )
    returned, mixed_out = lax.optimization_barrier((returned, mixed_out))
    returned = returned.reshape(slot_total, cols_part)
    picked0 = jnp.dot(pick0.astype(BF), returned, preferred_element_type=F32)
    picked1 = jnp.dot(pick1.astype(BF), returned, preferred_element_type=F32)
    expert_out = (
        picked0 * route_weights[:, 0:1] + picked1 * route_weights[:, 1:2]
    ).astype(BF)

    return (mixed_out, expert_out)


def solution(mesh):
    ep, tp = mesh.devices.shape
    fine = Mesh(mesh.devices.reshape(ep // 2, 2, tp), ("z", "c", "tp"))
    both = ("z", "c")
    return jax.shard_map(
        layer,
        mesh=fine,
        in_specs=(
            P("tp", both),
            P("tp", both),
            P("tp", both),
            P(),
            P(None, "tp"),
            P(both, "tp"),
            P(both, None),
            P(both, None),
            P(both, None, "tp"),
            P(both, None, "tp"),
            P(both, "tp", None),
        ),
        out_specs=(P(both, "tp"), P(both, "tp")),
        check_vma=False,
    )
```

```python
import functools

import jax
import jax.numpy as jnp
from jax import lax
from jax.experimental import pallas as pl
from jax.experimental.pallas import tpu as pltpu
from jax.sharding import Mesh
from jax.sharding import PartitionSpec as P

KERNEL = 3
EPSILON = 1e-06
BF = jnp.bfloat16
F32 = jnp.float32


def ones_where(test):
    return jnp.where(test, 1.0, 0.0).astype(BF)


def dispatch_kernel(me_ref, routes_ref, rows_ref, places_ref, out_ref, *, experts, tp):
    core = me_ref[0] // tp
    rows = rows_ref.shape[0]
    slot_total = out_ref.shape[0]
    capacity = slot_total // experts
    ids = lax.broadcasted_iota(jnp.int32, (rows, experts), 1)
    named = [routes_ref[:, k : k + 1] for k in range(2)]
    hit = [n == ids for n in named]
    later = lax.broadcasted_iota(jnp.int32, (rows, rows), 0)
    sooner = lax.broadcasted_iota(jnp.int32, (rows, rows), 1)
    earlier = jnp.dot(
        ones_where(sooner < later), ones_where(hit[0] | hit[1]), preferred_element_type=F32
    )
    slots = lax.broadcasted_iota(jnp.int32, (rows, slot_total), 1)
    taken = []
    for k in range(2):
        slot = jnp.sum(jnp.where(hit[k], earlier, 0.0), axis=1, keepdims=True)
        place = (named[k] ^ core) * capacity + slot.astype(jnp.int32)
        places_ref[:, k : k + 1] = place
        taken.append(place == slots)
    out_ref[...] = lax.dot_general(
        ones_where(taken[0] | taken[1]),
        rows_ref[...],
        (((0,), (0,)), ((), ())),
        preferred_element_type=F32,
    ).astype(BF)


def combine_kernel(places_ref, weights_ref, returned_ref, out_ref):
    rows = out_ref.shape[0]
    slots = lax.broadcasted_iota(jnp.int32, (rows, returned_ref.shape[0]), 1)
    total = None
    for k in range(2):
        pick = ones_where(places_ref[:, k : k + 1] == slots)
        picked = jnp.dot(pick, returned_ref[...], preferred_element_type=F32)
        term = picked * weights_ref[:, k : k + 1]
        total = term if total is None else total + term
    out_ref[...] = total.astype(BF)


def sum_kernel(in_ref, out_ref):
    total = in_ref[0].astype(F32)
    for j in range(1, in_ref.shape[0]):
        total = total + in_ref[j].astype(F32)
    out_ref[...] = total.astype(BF)


def expert_kernel(me_ref, x_ref, gate_ref, up_ref, down_ref, out_ref):
    parts = x_ref.shape[0]
    cols = x_ref.shape[2]
    side = 4
    core = me_ref[0] // parts
    natural = [j for j in range(parts)]
    turned = [(j % side) * side + j // side for j in range(parts)]
    store = [jnp.where(core == 0, turned[j], natural[j]) for j in range(parts)]
    x = jnp.concatenate([x_ref[j] for j in range(parts)], axis=1)
    values = x.astype(F32)
    squares = jnp.sum(values * values, axis=1, keepdims=True)
    scale = lax.rsqrt(squares / (parts * cols) + EPSILON)
    gate = scale * jnp.dot(x, gate_ref[...], preferred_element_type=F32)
    up = scale * jnp.dot(x, up_ref[...], preferred_element_type=F32)
    hidden = (jax.nn.silu(gate) * up).astype(BF)
    part = jnp.dot(hidden, down_ref[...], preferred_element_type=F32).astype(BF)
    for j in range(parts):
        out_ref[store[j]] = part[:, j * cols : (j + 1) * cols]


def expert_part(me, x, gate_weight, up_weight, down_weight, tile):
    parts, rows, cols = x.shape
    whole = lambda w: pl.BlockSpec(w.shape, lambda i, c: (0, 0))
    return pl.pallas_call(
        expert_kernel,
        grid_spec=pltpu.PrefetchScalarGridSpec(
            num_scalar_prefetch=1,
            grid=(rows // tile,),
            in_specs=[
                pl.BlockSpec((parts, tile, cols), lambda i, c: (0, i, 0)),
                whole(gate_weight),
                whole(up_weight),
                whole(down_weight),
            ],
            out_specs=pl.BlockSpec((parts, tile, cols), lambda i, c: (0, i, 0)),
        ),
        out_shape=jax.ShapeDtypeStruct(x.shape, BF),
        compiler_params=pltpu.CompilerParams(vmem_limit_bytes=28 * 1024 * 1024),
        cost_estimate=pl.CostEstimate(
            flops=6 * rows * parts * cols * gate_weight.shape[1],
            bytes_accessed=2 * 2 * rows * parts * cols + 6 * gate_weight.size,
            transcendentals=rows * gate_weight.shape[1],
        ),
    )(me.reshape(1), x, gate_weight, up_weight, down_weight)


def mixer_kernel(me_ref, y0_ref, y1_ref, y2a_ref, y2b_ref, y3_ref, proj_ref, out_ref):
    blocks = proj_ref.shape[0]
    side = 4
    core = me_ref[0] // blocks
    row = (me_ref[0] % blocks) // side
    col = me_ref[0] % side
    weights = []
    for far in range(side):
        for near in range(side):
            down = jnp.where(core == 0, far, near)
            right = jnp.where(core == 0, near, far)
            at = ((row + down) % side) * side + (col + right) % side
            weights.append(proj_ref[at])
    proj = jnp.concatenate(weights, axis=0)
    pieces = [
        ref[i]
        for ref in (y0_ref, y1_ref, y2a_ref, y2b_ref, y3_ref)
        for i in range(ref.shape[0])
    ]
    y = jnp.concatenate(pieces, axis=0)
    flat = lax.dot_general(
        proj, y, (((0,), (0,)), ((), ())), preferred_element_type=F32
    )
    out_ref[...] = jnp.transpose(flat).astype(BF)


def mixer_product(me, pieces, proj, tile):
    length = pieces[0].shape[2]
    blocks, width, cols = proj.shape
    return pl.pallas_call(
        mixer_kernel,
        grid_spec=pltpu.PrefetchScalarGridSpec(
            num_scalar_prefetch=1,
            grid=(length // tile,),
            in_specs=[
                pl.BlockSpec(p.shape[:2] + (tile,), lambda i, c: (0, 0, i)) for p in pieces
            ]
            + [pl.BlockSpec(proj.shape, lambda i, c: (0, 0, 0))],
            out_specs=pl.BlockSpec((tile, cols), lambda i, c: (i, 0)),
        ),
        out_shape=jax.ShapeDtypeStruct((length, cols), BF),
        compiler_params=pltpu.CompilerParams(vmem_limit_bytes=20 * 1024 * 1024),
        cost_estimate=pl.CostEstimate(
            flops=2 * length * blocks * width * cols,
            bytes_accessed=2 * length * (blocks * width + cols) + 2 * proj.size,
            transcendentals=0,
        ),
    )(me.reshape(1), *pieces, proj)


def sum_parts(arrived, steps):
    parts, rows, cols = arrived.shape
    return pl.pallas_call(
        sum_kernel,
        grid=(steps,),
        in_specs=[pl.BlockSpec((parts, rows // steps, cols), lambda i: (0, i, 0))],
        out_specs=pl.BlockSpec((rows // steps, cols), lambda i: (i, 0)),
        out_shape=jax.ShapeDtypeStruct((rows, cols), BF),
        compiler_params=pltpu.CompilerParams(vmem_limit_bytes=12 * 1024 * 1024),
    )(arrived)


def layer(
    conv_input,
    out_gate,
    in_gate,
    conv_taps,
    mixer_proj,
    token_rows,
    routes,
    route_weights,
    expert_gate,
    expert_up,
    expert_down,
):
    depth = lax.axis_size("z")
    experts = 2 * depth
    tp = lax.axis_size("tp")
    me = lax.axis_index(("c", "tp"))
    rows_b, cols_part = token_rows.shape
    capacity = 4 * rows_b // experts
    slot_total = experts * capacity
    half = slot_total // 2

    places, outgoing = pl.pallas_call(
        functools.partial(dispatch_kernel, experts=experts, tp=tp),
        grid_spec=pltpu.PrefetchScalarGridSpec(
            num_scalar_prefetch=1,
            grid=(1,),
            in_specs=[
                pl.BlockSpec(routes.shape, lambda i, c: (0, 0)),
                pl.BlockSpec(token_rows.shape, lambda i, c: (0, 0)),
            ],
            out_specs=[
                pl.BlockSpec(routes.shape, lambda i, c: (0, 0)),
                pl.BlockSpec((slot_total, cols_part), lambda i, c: (0, 0)),
            ],
        ),
        out_shape=[
            jax.ShapeDtypeStruct(routes.shape, jnp.int32),
            jax.ShapeDtypeStruct((slot_total, cols_part), BF),
        ],
        compiler_params=pltpu.CompilerParams(vmem_limit_bytes=12 * 1024 * 1024),
    )(me.reshape(1), routes, token_rows)
    outgoing, conv_input, in_gate = lax.optimization_barrier((outgoing, conv_input, in_gate))
    arrived = lax.all_to_all(
        outgoing.reshape(depth, 2, capacity, cols_part), "z", 0, 0, tiled=True
    )

    length = conv_input.shape[1]
    width_part = conv_input.shape[0]
    offset = lax.axis_index("tp") * width_part
    local_taps = lax.dynamic_slice_in_dim(conv_taps, offset, width_part, 1)
    z_rows = (conv_input.astype(F32) * in_gate.astype(F32)).astype(BF)
    pairs = [(i, i + 1) for i in range(experts - 1)]
    rim = lax.ppermute(z_rows[:, length - (KERNEL - 1) :], ("z", "c"), pairs)
    longer = jnp.concatenate([rim, z_rows], axis=1).astype(F32)
    conv_sum = jnp.zeros(z_rows.shape, F32)
    for lag in range(KERNEL):
        begin = KERNEL - 1 - lag
        conv_sum = conv_sum + local_taps[lag][:, None] * longer[:, begin : begin + length]
    gated = (out_gate.astype(F32) * conv_sum).astype(BF)
    side = 4
    swap = [(0, 1), (1, 0)]
    place = lambda c, y, x: (c * side + y) * side + x
    span = range(side)
    along_x = lambda c: [[place(c, y, x) for x in span] for y in span]
    along_y = lambda c: [[place(c, y, x) for y in span] for x in span]
    early = along_x(0) + along_y(1)
    late = along_y(0) + along_x(1)

    def step(value, by, phase):
        pairs = []
        for c in range(2):
            for y in span:
                for x in span:
                    if (c == 0) == (phase == 0):
                        to = place(c, y, (x + by) % side)
                    else:
                        to = place(c, (y + by) % side, x)
                    pairs.append((place(c, y, x), to))
        return lax.ppermute(value, ("c", "tp"), pairs)

    gated = gated.reshape(2, width_part // 2, length)
    before = step(gated, 1, 0)
    after = step(gated, -1, 0)
    far = step(gated, 2, 0)
    line = jnp.concatenate([gated, after, far, before], axis=0)
    arrived, line = lax.optimization_barrier((arrived, line))

    def exchange(value, groups):
        return lax.all_to_all(
            value, ("c", "tp"), 0, 0, axis_index_groups=groups, tiled=True
        )

    rows_own = arrived[:, 0].reshape(half, cols_part)
    rows_other = lax.ppermute(arrived[:, 1].reshape(half, cols_part), "c", swap)
    rows = jnp.concatenate([rows_own, rows_other], axis=0)
    x = lax.all_to_all(
        jnp.broadcast_to(rows[None], (tp,) + rows.shape), "tp", 0, 0, tiled=True
    )
    weights = (expert_gate[0], expert_up[0], expert_down[0])
    part = expert_part(me, x, *weights, rows_b)
    part = part.reshape(side, side, slot_total, cols_part)
    half_sums = exchange(part, early).reshape(side, side * slot_total, cols_part)
    half_sums = sum_parts(half_sums, 8).reshape(side, slot_total, cols_part)
    half_sums, line = lax.optimization_barrier((half_sums, line))
    line_before = step(line, 1, 1)
    line_after = step(line, -1, 1)
    expert_rows = exchange(half_sums, late)
    expert_rows = sum_parts(expert_rows, 2)
    back_own = expert_rows[:half]
    back_other = lax.ppermute(expert_rows[half:], "c", swap)
    back = jnp.stack(
        [
            back_own.reshape(depth, capacity, cols_part),
            back_other.reshape(depth, capacity, cols_part),
        ],
        axis=1,
    )
    line_far_a = step(line_before[:4], 1, 1)
    line_far_b = step(line_after[4:], -1, 1)
    returned = lax.all_to_all(back, "z", 0, 0, tiled=True)
    mixed_out = mixer_product(
        me,
        (line, line_after, line_far_a, line_far_b, line_before),
        mixer_proj.reshape(tp, width_part, cols_part),
        length // 4,
    )
    returned, mixed_out = lax.optimization_barrier((returned, mixed_out))
    returned = returned.reshape(slot_total, cols_part)
    expert_out = pl.pallas_call(
        combine_kernel,
        out_shape=jax.ShapeDtypeStruct((rows_b, cols_part), BF),
        compiler_params=pltpu.CompilerParams(vmem_limit_bytes=12 * 1024 * 1024),
    )(places, route_weights, returned)
    return (mixed_out, expert_out)


def solution(mesh):
    ep, tp = mesh.devices.shape
    fine = Mesh(mesh.devices.reshape(ep // 2, 2, tp), ("z", "c", "tp"))
    both = ("z", "c")
    return jax.shard_map(
        layer,
        mesh=fine,
        in_specs=(
            P("tp", both),
            P("tp", both),
            P("tp", both),
            P(),
            P(None, "tp"),
            P(both, "tp"),
            P(both, None),
            P(both, None),
            P(both, None, "tp"),
            P(both, None, "tp"),
            P(both, "tp", None),
        ),
        out_specs=(P(both, "tp"), P(both, "tp")),
        check_vma=False,
    )
```

```python
import functools

import jax
import jax.numpy as jnp
from jax import lax
from jax.experimental import pallas as pl
from jax.experimental.pallas import tpu as pltpu
from jax.sharding import Mesh
from jax.sharding import PartitionSpec as P

KERNEL = 3
EPSILON = 1e-06
BF = jnp.bfloat16
F32 = jnp.float32


def ones_where(test):
    return jnp.where(test, 1.0, 0.0).astype(BF)


def dispatch_kernel(me_ref, routes_ref, rows_ref, places_ref, out_ref, *, experts, tp):
    core = me_ref[0] // tp
    rows = rows_ref.shape[0]
    slot_total = out_ref.shape[0]
    capacity = slot_total // experts
    ids = lax.broadcasted_iota(jnp.int32, (rows, experts), 1)
    named = [routes_ref[:, k : k + 1] for k in range(2)]
    hit = [n == ids for n in named]
    later = lax.broadcasted_iota(jnp.int32, (rows, rows), 0)
    sooner = lax.broadcasted_iota(jnp.int32, (rows, rows), 1)
    earlier = jnp.dot(
        ones_where(sooner < later), ones_where(hit[0] | hit[1]), preferred_element_type=F32
    )
    slots = lax.broadcasted_iota(jnp.int32, (rows, slot_total), 1)
    taken = []
    for k in range(2):
        slot = jnp.sum(jnp.where(hit[k], earlier, 0.0), axis=1, keepdims=True)
        place = (named[k] ^ core) * capacity + slot.astype(jnp.int32)
        places_ref[:, k : k + 1] = place
        taken.append(place == slots)
    out_ref[...] = lax.dot_general(
        ones_where(taken[0] | taken[1]),
        rows_ref[...],
        (((0,), (0,)), ((), ())),
        preferred_element_type=F32,
    ).astype(BF)


def combine_kernel(places_ref, weights_ref, returned_ref, out_ref):
    rows = out_ref.shape[0]
    slots = lax.broadcasted_iota(jnp.int32, (rows, returned_ref.shape[0]), 1)
    total = None
    for k in range(2):
        pick = ones_where(places_ref[:, k : k + 1] == slots)
        picked = jnp.dot(pick, returned_ref[...], preferred_element_type=F32)
        term = picked * weights_ref[:, k : k + 1]
        total = term if total is None else total + term
    out_ref[...] = total.astype(BF)


def sum_kernel(in_ref, out_ref):
    total = in_ref[0].astype(F32)
    for j in range(1, in_ref.shape[0]):
        total = total + in_ref[j].astype(F32)
    out_ref[...] = total.astype(BF)


def expert_kernel(me_ref, x_ref, *refs):
    sources, (out_ref, gate_ref, up_ref, down_ref, sems) = refs[:3], refs[3:]
    copies = [
        pltpu.make_async_copy(source, target, sems.at[k])
        for k, (source, target) in enumerate(zip(sources, (gate_ref, up_ref, down_ref)))
    ]

    @pl.when(pl.program_id(0) == 0)
    def _():
        for copy in copies:
            copy.start()

    parts = x_ref.shape[0]
    cols = x_ref.shape[2]
    side = 4
    core = me_ref[0] // parts
    natural = [j for j in range(parts)]
    turned = [(j % side) * side + j // side for j in range(parts)]
    load = [jnp.where(core == 0, natural[j], turned[j]) for j in range(parts)]
    store = [jnp.where(core == 0, turned[j], natural[j]) for j in range(parts)]
    x = jnp.concatenate([x_ref[load[j]] for j in range(parts)], axis=1)
    values = x.astype(F32)
    squares = jnp.sum(values * values, axis=1, keepdims=True)
    scale = lax.rsqrt(squares / (parts * cols) + EPSILON)

    @pl.when(pl.program_id(0) == 0)
    def _():
        for copy in copies:
            copy.wait()

    gate = scale * jnp.dot(x, gate_ref[...], preferred_element_type=F32)
    up = scale * jnp.dot(x, up_ref[...], preferred_element_type=F32)
    hidden = (jax.nn.silu(gate) * up).astype(BF)
    part = jnp.dot(hidden, down_ref[...], preferred_element_type=F32).astype(BF)
    for j in range(parts):
        out_ref[store[j]] = part[:, j * cols : (j + 1) * cols]


def expert_part(me, x, gate_weight, up_weight, down_weight, tile):
    parts, rows, cols = x.shape
    stays = pl.BlockSpec(memory_space=pltpu.HBM)
    return pl.pallas_call(
        expert_kernel,
        grid_spec=pltpu.PrefetchScalarGridSpec(
            num_scalar_prefetch=1,
            grid=(rows // tile,),
            in_specs=[
                pl.BlockSpec((parts, tile, cols), lambda i, c: (0, i, 0)),
                stays,
                stays,
                stays,
            ],
            out_specs=pl.BlockSpec((parts, tile, cols), lambda i, c: (0, i, 0)),
            scratch_shapes=[
                pltpu.VMEM(gate_weight.shape, BF),
                pltpu.VMEM(up_weight.shape, BF),
                pltpu.VMEM(down_weight.shape, BF),
                pltpu.SemaphoreType.DMA((3,)),
            ],
        ),
        out_shape=jax.ShapeDtypeStruct(x.shape, BF),
        compiler_params=pltpu.CompilerParams(vmem_limit_bytes=28 * 1024 * 1024),
        cost_estimate=pl.CostEstimate(
            flops=6 * rows * parts * cols * gate_weight.shape[1],
            bytes_accessed=2 * 2 * rows * parts * cols + 6 * gate_weight.size,
            transcendentals=rows * gate_weight.shape[1],
        ),
    )(me.reshape(1), x, gate_weight, up_weight, down_weight)


def mixer_kernel(me_ref, y0_ref, y1_ref, y2a_ref, y2b_ref, y3_ref, proj_ref, out_ref):
    blocks = proj_ref.shape[0]
    side = 4
    core = me_ref[0] // blocks
    row = (me_ref[0] % blocks) // side
    col = me_ref[0] % side
    weights = []
    for far in range(side):
        for near in range(side):
            down = jnp.where(core == 0, far, near)
            right = jnp.where(core == 0, near, far)
            at = ((row + down) % side) * side + (col + right) % side
            weights.append(proj_ref[at])
    proj = jnp.concatenate(weights, axis=0)
    pieces = [
        ref[i]
        for ref in (y0_ref, y1_ref, y2a_ref, y2b_ref, y3_ref)
        for i in range(ref.shape[0])
    ]
    y = jnp.concatenate(pieces, axis=0)
    flat = lax.dot_general(
        proj, y, (((0,), (0,)), ((), ())), preferred_element_type=F32
    )
    out_ref[...] = jnp.transpose(flat).astype(BF)


def mixer_product(me, pieces, proj, tile):
    length = pieces[0].shape[2]
    blocks, width, cols = proj.shape
    return pl.pallas_call(
        mixer_kernel,
        grid_spec=pltpu.PrefetchScalarGridSpec(
            num_scalar_prefetch=1,
            grid=(length // tile,),
            in_specs=[
                pl.BlockSpec(p.shape[:2] + (tile,), lambda i, c: (0, 0, i)) for p in pieces
            ]
            + [pl.BlockSpec(proj.shape, lambda i, c: (0, 0, 0))],
            out_specs=pl.BlockSpec((tile, cols), lambda i, c: (i, 0)),
        ),
        out_shape=jax.ShapeDtypeStruct((length, cols), BF),
        compiler_params=pltpu.CompilerParams(vmem_limit_bytes=20 * 1024 * 1024),
        cost_estimate=pl.CostEstimate(
            flops=2 * length * blocks * width * cols,
            bytes_accessed=2 * length * (blocks * width + cols) + 2 * proj.size,
            transcendentals=0,
        ),
    )(me.reshape(1), *pieces, proj)


def sum_parts(arrived, steps):
    parts, rows, cols = arrived.shape
    return pl.pallas_call(
        sum_kernel,
        grid=(steps,),
        in_specs=[pl.BlockSpec((parts, rows // steps, cols), lambda i: (0, i, 0))],
        out_specs=pl.BlockSpec((rows // steps, cols), lambda i: (i, 0)),
        out_shape=jax.ShapeDtypeStruct((rows, cols), BF),
        compiler_params=pltpu.CompilerParams(vmem_limit_bytes=12 * 1024 * 1024),
    )(arrived)


def layer(
    conv_input,
    out_gate,
    in_gate,
    conv_taps,
    mixer_proj,
    token_rows,
    routes,
    route_weights,
    expert_gate,
    expert_up,
    expert_down,
):
    depth = lax.axis_size("z")
    experts = 2 * depth
    tp = lax.axis_size("tp")
    me = lax.axis_index(("c", "tp"))
    rows_b, cols_part = token_rows.shape
    capacity = 4 * rows_b // experts
    slot_total = experts * capacity
    half = slot_total // 2

    places, outgoing = pl.pallas_call(
        functools.partial(dispatch_kernel, experts=experts, tp=tp),
        grid_spec=pltpu.PrefetchScalarGridSpec(
            num_scalar_prefetch=1,
            grid=(1,),
            in_specs=[
                pl.BlockSpec(routes.shape, lambda i, c: (0, 0)),
                pl.BlockSpec(token_rows.shape, lambda i, c: (0, 0)),
            ],
            out_specs=[
                pl.BlockSpec(routes.shape, lambda i, c: (0, 0)),
                pl.BlockSpec((slot_total, cols_part), lambda i, c: (0, 0)),
            ],
        ),
        out_shape=[
            jax.ShapeDtypeStruct(routes.shape, jnp.int32),
            jax.ShapeDtypeStruct((slot_total, cols_part), BF),
        ],
        compiler_params=pltpu.CompilerParams(vmem_limit_bytes=12 * 1024 * 1024),
    )(me.reshape(1), routes, token_rows)
    outgoing, conv_input, in_gate = lax.optimization_barrier((outgoing, conv_input, in_gate))
    arrived = lax.all_to_all(
        outgoing.reshape(depth, 2, capacity, cols_part), "z", 0, 0, tiled=True
    )

    length = conv_input.shape[1]
    width_part = conv_input.shape[0]
    offset = lax.axis_index("tp") * width_part
    local_taps = lax.dynamic_slice_in_dim(conv_taps, offset, width_part, 1)
    z_rows = (conv_input.astype(F32) * in_gate.astype(F32)).astype(BF)
    pairs = [(i, i + 1) for i in range(experts - 1)]
    rim = lax.ppermute(z_rows[:, length - (KERNEL - 1) :], ("z", "c"), pairs)
    longer = jnp.concatenate([rim, z_rows], axis=1).astype(F32)
    conv_sum = jnp.zeros(z_rows.shape, F32)
    for lag in range(KERNEL):
        begin = KERNEL - 1 - lag
        conv_sum = conv_sum + local_taps[lag][:, None] * longer[:, begin : begin + length]
    gated = (out_gate.astype(F32) * conv_sum).astype(BF)
    side = 4
    swap = [(0, 1), (1, 0)]
    place = lambda c, y, x: (c * side + y) * side + x
    span = range(side)
    along_x = lambda c: [[place(c, y, x) for x in span] for y in span]
    along_y = lambda c: [[place(c, y, x) for y in span] for x in span]
    early = along_x(0) + along_y(1)
    late = along_y(0) + along_x(1)

    def step(value, by, phase):
        pairs = []
        for c in range(2):
            for y in span:
                for x in span:
                    if (c == 0) == (phase == 0):
                        to = place(c, y, (x + by) % side)
                    else:
                        to = place(c, (y + by) % side, x)
                    pairs.append((place(c, y, x), to))
        return lax.ppermute(value, ("c", "tp"), pairs)

    gated = gated.reshape(2, width_part // 2, length)
    before = step(gated, 1, 0)
    after = step(gated, -1, 0)
    far = step(gated, 2, 0)
    line = jnp.concatenate([gated, after, far, before], axis=0)
    arrived, line = lax.optimization_barrier((arrived, line))

    def exchange(value, groups):
        return lax.all_to_all(
            value, ("c", "tp"), 0, 0, axis_index_groups=groups, tiled=True
        )

    rows_own = arrived[:, 0].reshape(half, cols_part)
    rows_other = lax.ppermute(arrived[:, 1].reshape(half, cols_part), "c", swap)
    rows = jnp.concatenate([rows_own, rows_other], axis=0)
    quarter = exchange(jnp.broadcast_to(rows[None], (side,) + rows.shape), early)
    line_before = step(line, 1, 1)
    line_after = step(line, -1, 1)
    quarter, line_before, line_after = lax.optimization_barrier(
        (quarter, line_before, line_after)
    )
    x = exchange(jnp.broadcast_to(quarter[None], (side,) + quarter.shape), late)
    line_far_a = step(line_before[:4], 1, 1)
    line_far_b = step(line_after[4:], -1, 1)
    mixed_out = mixer_product(
        me,
        (line, line_after, line_far_a, line_far_b, line_before),
        mixer_proj.reshape(tp, width_part, cols_part),
        length // 4,
    )
    x, mixed_out = lax.optimization_barrier((x, mixed_out))
    x = x.reshape(tp, slot_total, cols_part)
    weights = (expert_gate[0], expert_up[0], expert_down[0])
    part = expert_part(me, x, *weights, rows_b)
    part = part.reshape(side, side, slot_total, cols_part)
    half_sums = exchange(part, early).reshape(side, side * slot_total, cols_part)
    half_sums = sum_parts(half_sums, 8).reshape(side, slot_total, cols_part)
    expert_rows = sum_parts(exchange(half_sums, late), 2)
    back_own = expert_rows[:half]
    back_other = lax.ppermute(expert_rows[half:], "c", swap)
    back = jnp.stack(
        [
            back_own.reshape(depth, capacity, cols_part),
            back_other.reshape(depth, capacity, cols_part),
        ],
        axis=1,
    )
    returned = lax.all_to_all(back, "z", 0, 0, tiled=True)
    returned = returned.reshape(slot_total, cols_part)
    expert_out = pl.pallas_call(
        combine_kernel,
        out_shape=jax.ShapeDtypeStruct((rows_b, cols_part), BF),
        compiler_params=pltpu.CompilerParams(vmem_limit_bytes=12 * 1024 * 1024),
    )(places, route_weights, returned)
    return (mixed_out, expert_out)


def solution(mesh):
    ep, tp = mesh.devices.shape
    fine = Mesh(mesh.devices.reshape(ep // 2, 2, tp), ("z", "c", "tp"))
    both = ("z", "c")
    return jax.shard_map(
        layer,
        mesh=fine,
        in_specs=(
            P("tp", both),
            P("tp", both),
            P("tp", both),
            P(),
            P(None, "tp"),
            P(both, "tp"),
            P(both, None),
            P(both, None),
            P(both, None, "tp"),
            P(both, None, "tp"),
            P(both, "tp", None),
        ),
        out_specs=(P(both, "tp"), P(both, "tp")),
        check_vma=False,
    )
```

```python
import functools

import jax
import jax.numpy as jnp
from jax import lax
from jax.experimental import pallas as pl
from jax.experimental.pallas import tpu as pltpu
from jax.sharding import Mesh
from jax.sharding import PartitionSpec as P

KERNEL = 3
EPSILON = 1e-06
BF = jnp.bfloat16
F32 = jnp.float32


def ones_where(test):
    return jnp.where(test, 1.0, 0.0).astype(BF)


def dispatch_kernel(me_ref, routes_ref, rows_ref, places_ref, out_ref, *, experts, tp):
    core = me_ref[0] // tp
    rows = rows_ref.shape[0]
    slot_total = out_ref.shape[0]
    capacity = slot_total // experts
    ids = lax.broadcasted_iota(jnp.int32, (experts, rows), 0)
    named = [routes_ref[k : k + 1, :] for k in range(2)]
    hit = [n == ids for n in named]
    sooner = lax.broadcasted_iota(jnp.int32, (rows, rows), 0)
    later = lax.broadcasted_iota(jnp.int32, (rows, rows), 1)
    earlier = jnp.dot(
        ones_where(hit[0] | hit[1]), ones_where(sooner < later), preferred_element_type=F32
    )
    slots = lax.broadcasted_iota(jnp.int32, (slot_total, rows), 0)
    taken = []
    for k in range(2):
        slot = jnp.sum(jnp.where(hit[k], earlier, 0.0), axis=0, keepdims=True)
        place = (named[k] ^ core) * capacity + slot.astype(jnp.int32)
        places_ref[k : k + 1, :] = place
        taken.append(place == slots)
    out_ref[...] = jnp.dot(
        ones_where(taken[0] | taken[1]), rows_ref[...], preferred_element_type=F32
    ).astype(BF)


def combine_kernel(places_ref, weights_ref, returned_ref, out_ref):
    rows = out_ref.shape[0]
    slots = lax.broadcasted_iota(jnp.int32, (returned_ref.shape[0], rows), 0)
    total = None
    for k in range(2):
        pick = ones_where(places_ref[k : k + 1, :] == slots)
        picked = lax.dot_general(
            pick, returned_ref[...], (((0,), (0,)), ((), ())), preferred_element_type=F32
        )
        term = picked * weights_ref[:, k : k + 1]
        total = term if total is None else total + term
    out_ref[...] = total.astype(BF)


def sum_kernel(in_ref, out_ref):
    total = in_ref[0].astype(F32)
    for j in range(1, in_ref.shape[0]):
        total = total + in_ref[j].astype(F32)
    out_ref[...] = total.astype(BF)


def expert_kernel(me_ref, x_ref, gate_ref, up_ref, down_ref, out_ref):
    parts = x_ref.shape[0]
    cols = x_ref.shape[2]
    side = 4
    core = me_ref[0] // parts
    natural = [j for j in range(parts)]
    turned = [(j % side) * side + j // side for j in range(parts)]
    load = [jnp.where(core == 0, natural[j], turned[j]) for j in range(parts)]
    store = [jnp.where(core == 0, turned[j], natural[j]) for j in range(parts)]
    x = jnp.concatenate([x_ref[load[j]] for j in range(parts)], axis=1)
    values = x.astype(F32)
    squares = jnp.sum(values * values, axis=1, keepdims=True)
    scale = lax.rsqrt(squares / (parts * cols) + EPSILON)
    gate = scale * jnp.dot(x, gate_ref[...], preferred_element_type=F32)
    up = scale * jnp.dot(x, up_ref[...], preferred_element_type=F32)
    hidden = (jax.nn.silu(gate) * up).astype(BF)
    part = jnp.dot(hidden, down_ref[...], preferred_element_type=F32).astype(BF)
    for j in range(parts):
        out_ref[store[j]] = part[:, j * cols : (j + 1) * cols]


def expert_part(me, x, gate_weight, up_weight, down_weight, tile):
    parts, rows, cols = x.shape
    whole = lambda w: pl.BlockSpec(w.shape, lambda i, c: (0, 0))
    return pl.pallas_call(
        expert_kernel,
        grid_spec=pltpu.PrefetchScalarGridSpec(
            num_scalar_prefetch=1,
            grid=(rows // tile,),
            in_specs=[
                pl.BlockSpec((parts, tile, cols), lambda i, c: (0, i, 0)),
                whole(gate_weight),
                whole(up_weight),
                whole(down_weight),
            ],
            out_specs=pl.BlockSpec((parts, tile, cols), lambda i, c: (0, i, 0)),
        ),
        out_shape=jax.ShapeDtypeStruct(x.shape, BF),
        compiler_params=pltpu.CompilerParams(vmem_limit_bytes=28 * 1024 * 1024),
        cost_estimate=pl.CostEstimate(
            flops=6 * rows * parts * cols * gate_weight.shape[1],
            bytes_accessed=2 * 2 * rows * parts * cols + 6 * gate_weight.size,
            transcendentals=rows * gate_weight.shape[1],
        ),
    )(me.reshape(1), x, gate_weight, up_weight, down_weight)


def mixer_kernel(me_ref, y0_ref, y1_ref, y2a_ref, y2b_ref, y3_ref, proj_ref, out_ref):
    blocks = proj_ref.shape[0]
    side = 4
    core = me_ref[0] // blocks
    row = (me_ref[0] % blocks) // side
    col = me_ref[0] % side
    weights = []
    for far in range(side):
        for near in range(side):
            down = jnp.where(core == 0, far, near)
            right = jnp.where(core == 0, near, far)
            at = ((row + down) % side) * side + (col + right) % side
            weights.append(proj_ref[at])
    proj = jnp.concatenate(weights, axis=0)
    pieces = [
        ref[i]
        for ref in (y0_ref, y1_ref, y2a_ref, y2b_ref, y3_ref)
        for i in range(ref.shape[0])
    ]
    y = jnp.concatenate(pieces, axis=0)
    flat = lax.dot_general(
        proj, y, (((0,), (0,)), ((), ())), preferred_element_type=F32
    )
    out_ref[...] = jnp.transpose(flat).astype(BF)


def mixer_product(me, pieces, proj, tile):
    length = pieces[0].shape[2]
    blocks, width, cols = proj.shape
    return pl.pallas_call(
        mixer_kernel,
        grid_spec=pltpu.PrefetchScalarGridSpec(
            num_scalar_prefetch=1,
            grid=(length // tile,),
            in_specs=[
                pl.BlockSpec(p.shape[:2] + (tile,), lambda i, c: (0, 0, i)) for p in pieces
            ]
            + [pl.BlockSpec(proj.shape, lambda i, c: (0, 0, 0))],
            out_specs=pl.BlockSpec((tile, cols), lambda i, c: (i, 0)),
        ),
        out_shape=jax.ShapeDtypeStruct((length, cols), BF),
        compiler_params=pltpu.CompilerParams(vmem_limit_bytes=20 * 1024 * 1024),
        cost_estimate=pl.CostEstimate(
            flops=2 * length * blocks * width * cols,
            bytes_accessed=2 * length * (blocks * width + cols) + 2 * proj.size,
            transcendentals=0,
        ),
    )(me.reshape(1), *pieces, proj)


def sum_parts(arrived, steps):
    parts, rows, cols = arrived.shape
    return pl.pallas_call(
        sum_kernel,
        grid=(steps,),
        in_specs=[pl.BlockSpec((parts, rows // steps, cols), lambda i: (0, i, 0))],
        out_specs=pl.BlockSpec((rows // steps, cols), lambda i: (i, 0)),
        out_shape=jax.ShapeDtypeStruct((rows, cols), BF),
        compiler_params=pltpu.CompilerParams(vmem_limit_bytes=12 * 1024 * 1024),
    )(arrived)


def layer(
    conv_input,
    out_gate,
    in_gate,
    conv_taps,
    mixer_proj,
    token_rows,
    routes,
    route_weights,
    expert_gate,
    expert_up,
    expert_down,
):
    depth = lax.axis_size("z")
    experts = 2 * depth
    tp = lax.axis_size("tp")
    me = lax.axis_index(("c", "tp"))
    rows_b, cols_part = token_rows.shape
    capacity = 4 * rows_b // experts
    slot_total = experts * capacity
    half = slot_total // 2

    by_choice = routes.T
    places, outgoing = pl.pallas_call(
        functools.partial(dispatch_kernel, experts=experts, tp=tp),
        grid_spec=pltpu.PrefetchScalarGridSpec(
            num_scalar_prefetch=1,
            grid=(1,),
            in_specs=[
                pl.BlockSpec(by_choice.shape, lambda i, c: (0, 0)),
                pl.BlockSpec(token_rows.shape, lambda i, c: (0, 0)),
            ],
            out_specs=[
                pl.BlockSpec(by_choice.shape, lambda i, c: (0, 0)),
                pl.BlockSpec((slot_total, cols_part), lambda i, c: (0, 0)),
            ],
        ),
        out_shape=[
            jax.ShapeDtypeStruct(by_choice.shape, jnp.int32),
            jax.ShapeDtypeStruct((slot_total, cols_part), BF),
        ],
        compiler_params=pltpu.CompilerParams(vmem_limit_bytes=12 * 1024 * 1024),
    )(me.reshape(1), by_choice, token_rows)
    outgoing, conv_input, in_gate = lax.optimization_barrier((outgoing, conv_input, in_gate))
    arrived = lax.all_to_all(
        outgoing.reshape(depth, 2, capacity, cols_part), "z", 0, 0, tiled=True
    )

    length = conv_input.shape[1]
    width_part = conv_input.shape[0]
    offset = lax.axis_index("tp") * width_part
    local_taps = lax.dynamic_slice_in_dim(conv_taps, offset, width_part, 1)
    z_rows = (conv_input.astype(F32) * in_gate.astype(F32)).astype(BF)
    pairs = [(i, i + 1) for i in range(experts - 1)]
    rim = lax.ppermute(z_rows[:, length - (KERNEL - 1) :], ("z", "c"), pairs)
    longer = jnp.concatenate([rim, z_rows], axis=1).astype(F32)
    conv_sum = jnp.zeros(z_rows.shape, F32)
    for lag in range(KERNEL):
        begin = KERNEL - 1 - lag
        conv_sum = conv_sum + local_taps[lag][:, None] * longer[:, begin : begin + length]
    gated = (out_gate.astype(F32) * conv_sum).astype(BF)
    side = 4
    swap = [(0, 1), (1, 0)]
    place = lambda c, y, x: (c * side + y) * side + x
    span = range(side)
    along_x = lambda c: [[place(c, y, x) for x in span] for y in span]
    along_y = lambda c: [[place(c, y, x) for y in span] for x in span]
    early = along_x(0) + along_y(1)
    late = along_y(0) + along_x(1)

    def step(value, by, phase):
        pairs = []
        for c in range(2):
            for y in span:
                for x in span:
                    if (c == 0) == (phase == 0):
                        to = place(c, y, (x + by) % side)
                    else:
                        to = place(c, (y + by) % side, x)
                    pairs.append((place(c, y, x), to))
        return lax.ppermute(value, ("c", "tp"), pairs)

    gated = gated.reshape(2, width_part // 2, length)
    before = step(gated, 1, 0)
    after = step(gated, -1, 0)
    far = step(gated, 2, 0)
    line = jnp.concatenate([gated, after, far, before], axis=0)

    def exchange(value, groups):
        return lax.all_to_all(
            value, ("c", "tp"), 0, 0, axis_index_groups=groups, tiled=True
        )

    rows_own = arrived[:, 0].reshape(half, cols_part)
    rows_other = lax.ppermute(arrived[:, 1].reshape(half, cols_part), "c", swap)
    rows = jnp.concatenate([rows_own, rows_other], axis=0)
    quarter = exchange(jnp.broadcast_to(rows[None], (side,) + rows.shape), early)
    quarter, line = lax.optimization_barrier((quarter, line))
    x = exchange(jnp.broadcast_to(quarter[None], (side,) + quarter.shape), late)
    x = x.reshape(tp, slot_total, cols_part)
    weights = (expert_gate[0], expert_up[0], expert_down[0])
    part = expert_part(me, x, *weights, rows_b)
    part = part.reshape(side, side, slot_total, cols_part)
    half_sums = exchange(part, early).reshape(side, side * slot_total, cols_part)
    half_sums = sum_parts(half_sums, 8).reshape(side, slot_total, cols_part)
    half_sums, line = lax.optimization_barrier((half_sums, line))
    line_before = step(line, 1, 1)
    line_after = step(line, -1, 1)
    expert_rows = exchange(half_sums, late)
    expert_rows = sum_parts(expert_rows, 2)
    back_own = expert_rows[:half]
    back_other = lax.ppermute(expert_rows[half:], "c", swap)
    back = jnp.stack(
        [
            back_own.reshape(depth, capacity, cols_part),
            back_other.reshape(depth, capacity, cols_part),
        ],
        axis=1,
    )
    line_far_a = step(line_before[:4], 1, 1)
    line_far_b = step(line_after[4:], -1, 1)
    returned = lax.all_to_all(back, "z", 0, 0, tiled=True)
    mixed_out = mixer_product(
        me,
        (line, line_after, line_far_a, line_far_b, line_before),
        mixer_proj.reshape(tp, width_part, cols_part),
        length // 4,
    )
    returned, mixed_out = lax.optimization_barrier((returned, mixed_out))
    returned = returned.reshape(slot_total, cols_part)
    expert_out = pl.pallas_call(
        combine_kernel,
        out_shape=jax.ShapeDtypeStruct((rows_b, cols_part), BF),
        compiler_params=pltpu.CompilerParams(vmem_limit_bytes=12 * 1024 * 1024),
    )(places, route_weights, returned)
    return (mixed_out, expert_out)


def solution(mesh):
    ep, tp = mesh.devices.shape
    fine = Mesh(mesh.devices.reshape(ep // 2, 2, tp), ("z", "c", "tp"))
    both = ("z", "c")
    return jax.shard_map(
        layer,
        mesh=fine,
        in_specs=(
            P("tp", both),
            P("tp", both),
            P("tp", both),
            P(),
            P(None, "tp"),
            P(both, "tp"),
            P(both, None),
            P(both, None),
            P(both, None, "tp"),
            P(both, None, "tp"),
            P(both, "tp", None),
        ),
        out_specs=(P(both, "tp"), P(both, "tp")),
        check_vma=False,
    )
```

```python
import functools

import jax
import jax.numpy as jnp
from jax import lax
from jax.experimental import pallas as pl
from jax.experimental.pallas import tpu as pltpu
from jax.sharding import Mesh
from jax.sharding import PartitionSpec as P

KERNEL = 3
EPSILON = 1e-06
BF = jnp.bfloat16
F32 = jnp.float32


def ones_where(test):
    return jnp.where(test, 1.0, 0.0).astype(BF)


def dispatch_kernel(me_ref, routes_ref, rows_ref, places_ref, out_ref, *, experts, tp):
    core = me_ref[0] // tp
    rows = rows_ref.shape[0]
    slot_total = out_ref.shape[0]
    capacity = slot_total // experts
    ids = lax.broadcasted_iota(jnp.int32, (experts, rows), 0)
    named = [routes_ref[k : k + 1, :] for k in range(2)]
    hit = [n == ids for n in named]
    sooner = lax.broadcasted_iota(jnp.int32, (rows, rows), 0)
    later = lax.broadcasted_iota(jnp.int32, (rows, rows), 1)
    earlier = jnp.dot(
        ones_where(hit[0] | hit[1]), ones_where(sooner < later), preferred_element_type=F32
    )
    slots = lax.broadcasted_iota(jnp.int32, (slot_total, rows), 0)
    taken = []
    for k in range(2):
        slot = jnp.sum(jnp.where(hit[k], earlier, 0.0), axis=0, keepdims=True)
        place = (named[k] ^ core) * capacity + slot.astype(jnp.int32)
        places_ref[k : k + 1, :] = place
        taken.append(place == slots)
    out_ref[...] = jnp.dot(
        ones_where(taken[0] | taken[1]), rows_ref[...], preferred_element_type=F32
    ).astype(BF)


def combine_kernel(places_ref, weights_ref, returned_ref, out_ref):
    rows = out_ref.shape[0]
    slots = lax.broadcasted_iota(jnp.int32, (returned_ref.shape[0], rows), 0)
    total = None
    for k in range(2):
        pick = ones_where(places_ref[k : k + 1, :] == slots)
        picked = lax.dot_general(
            pick, returned_ref[...], (((0,), (0,)), ((), ())), preferred_element_type=F32
        )
        term = picked * weights_ref[:, k : k + 1]
        total = term if total is None else total + term
    out_ref[...] = total.astype(BF)


def sum_kernel(in_ref, out_ref):
    total = in_ref[0].astype(F32)
    for j in range(1, in_ref.shape[0]):
        total = total + in_ref[j].astype(F32)
    out_ref[...] = total.astype(BF)


def expert_kernel(me_ref, x_ref, gate_ref, up_ref, down_ref, out_ref):
    parts = x_ref.shape[0]
    cols = x_ref.shape[2]
    side = 4
    core = me_ref[0] // parts
    natural = [j for j in range(parts)]
    turned = [(j % side) * side + j // side for j in range(parts)]
    load = [jnp.where(core == 0, natural[j], turned[j]) for j in range(parts)]
    store = [jnp.where(core == 0, turned[j], natural[j]) for j in range(parts)]
    x = jnp.concatenate([x_ref[load[j]] for j in range(parts)], axis=1)
    values = x.astype(F32)
    squares = jnp.sum(values * values, axis=1, keepdims=True)
    scale = lax.rsqrt(squares / (parts * cols) + EPSILON)
    gate = scale * jnp.dot(x, gate_ref[...], preferred_element_type=F32)
    up = scale * jnp.dot(x, up_ref[...], preferred_element_type=F32)
    hidden = (jax.nn.silu(gate) * up).astype(BF)
    part = jnp.dot(hidden, down_ref[...], preferred_element_type=F32).astype(BF)
    for j in range(parts):
        out_ref[store[j]] = part[:, j * cols : (j + 1) * cols]


def expert_part(me, x, gate_weight, up_weight, down_weight, tile):
    parts, rows, cols = x.shape
    whole = lambda w: pl.BlockSpec(w.shape, lambda i, c: (0, 0))
    return pl.pallas_call(
        expert_kernel,
        grid_spec=pltpu.PrefetchScalarGridSpec(
            num_scalar_prefetch=1,
            grid=(rows // tile,),
            in_specs=[
                pl.BlockSpec((parts, tile, cols), lambda i, c: (0, i, 0)),
                whole(gate_weight),
                whole(up_weight),
                whole(down_weight),
            ],
            out_specs=pl.BlockSpec((parts, tile, cols), lambda i, c: (0, i, 0)),
        ),
        out_shape=jax.ShapeDtypeStruct(x.shape, BF),
        compiler_params=pltpu.CompilerParams(vmem_limit_bytes=28 * 1024 * 1024),
        cost_estimate=pl.CostEstimate(
            flops=6 * rows * parts * cols * gate_weight.shape[1],
            bytes_accessed=2 * 2 * rows * parts * cols + 6 * gate_weight.size,
            transcendentals=rows * gate_weight.shape[1],
        ),
    )(me.reshape(1), x, gate_weight, up_weight, down_weight)


def mixer_kernel(me_ref, *refs, fars, last):
    refs, out_ref = refs[:-1], refs[-1]
    proj_ref, refs = refs[0], refs[1:]
    blocks = proj_ref.shape[0]
    side = 4
    core = me_ref[0] // blocks
    row = (me_ref[0] % blocks) // side
    col = me_ref[0] % side
    weights = []
    for far in fars:
        for near in range(side):
            down = jnp.where(core == 0, far, near)
            right = jnp.where(core == 0, near, far)
            at = ((row + down) % side) * side + (col + right) % side
            weights.append(proj_ref[at])
    proj = jnp.concatenate(weights, axis=0)
    pieces = refs[:-1] if last else refs
    y = jnp.concatenate([ref[i] for ref in pieces for i in range(ref.shape[0])], axis=0)
    flat = lax.dot_general(
        proj, y, (((0,), (0,)), ((), ())), preferred_element_type=F32
    )
    if last:
        out_ref[...] = jnp.transpose(flat + refs[-1][...]).astype(BF)
    else:
        out_ref[...] = flat


def mixer_product(me, proj, pieces, fars, base, tile):
    length = pieces[0].shape[2]
    _, width, cols = proj.shape
    last = base is not None
    flat_spec = pl.BlockSpec((cols, tile), lambda i, c: (0, i))
    return pl.pallas_call(
        functools.partial(mixer_kernel, fars=fars, last=last),
        grid_spec=pltpu.PrefetchScalarGridSpec(
            num_scalar_prefetch=1,
            grid=(length // tile,),
            in_specs=[pl.BlockSpec(proj.shape, lambda i, c: (0, 0, 0))]
            + [
                pl.BlockSpec(p.shape[:2] + (tile,), lambda i, c: (0, 0, i)) for p in pieces
            ]
            + ([flat_spec] if last else []),
            out_specs=pl.BlockSpec((tile, cols), lambda i, c: (i, 0)) if last else flat_spec,
        ),
        out_shape=jax.ShapeDtypeStruct((length, cols), BF)
        if last
        else jax.ShapeDtypeStruct((cols, length), F32),
        compiler_params=pltpu.CompilerParams(vmem_limit_bytes=16 * 1024 * 1024),
        cost_estimate=pl.CostEstimate(
            flops=2 * length * len(fars) * 4 * width * cols,
            bytes_accessed=2 * length * (len(fars) * 4 * width + 2 * cols) + 2 * proj.size,
            transcendentals=0,
        ),
    )(me.reshape(1), proj, *pieces, *([base] if last else []))


def sum_parts(arrived, steps):
    parts, rows, cols = arrived.shape
    return pl.pallas_call(
        sum_kernel,
        grid=(steps,),
        in_specs=[pl.BlockSpec((parts, rows // steps, cols), lambda i: (0, i, 0))],
        out_specs=pl.BlockSpec((rows // steps, cols), lambda i: (i, 0)),
        out_shape=jax.ShapeDtypeStruct((rows, cols), BF),
        compiler_params=pltpu.CompilerParams(vmem_limit_bytes=12 * 1024 * 1024),
    )(arrived)


def layer(
    conv_input,
    out_gate,
    in_gate,
    conv_taps,
    mixer_proj,
    token_rows,
    routes,
    route_weights,
    expert_gate,
    expert_up,
    expert_down,
):
    depth = lax.axis_size("z")
    experts = 2 * depth
    tp = lax.axis_size("tp")
    me = lax.axis_index(("c", "tp"))
    rows_b, cols_part = token_rows.shape
    capacity = 4 * rows_b // experts
    slot_total = experts * capacity
    half = slot_total // 2

    by_choice = routes.T
    places, outgoing = pl.pallas_call(
        functools.partial(dispatch_kernel, experts=experts, tp=tp),
        grid_spec=pltpu.PrefetchScalarGridSpec(
            num_scalar_prefetch=1,
            grid=(1,),
            in_specs=[
                pl.BlockSpec(by_choice.shape, lambda i, c: (0, 0)),
                pl.BlockSpec(token_rows.shape, lambda i, c: (0, 0)),
            ],
            out_specs=[
                pl.BlockSpec(by_choice.shape, lambda i, c: (0, 0)),
                pl.BlockSpec((slot_total, cols_part), lambda i, c: (0, 0)),
            ],
        ),
        out_shape=[
            jax.ShapeDtypeStruct(by_choice.shape, jnp.int32),
            jax.ShapeDtypeStruct((slot_total, cols_part), BF),
        ],
        compiler_params=pltpu.CompilerParams(vmem_limit_bytes=12 * 1024 * 1024),
    )(me.reshape(1), by_choice, token_rows)
    outgoing, conv_input, in_gate = lax.optimization_barrier((outgoing, conv_input, in_gate))
    arrived = lax.all_to_all(outgoing.reshape(depth, 2, capacity, cols_part), "z", 0, 0, tiled=True)

    length = conv_input.shape[1]
    width_part = conv_input.shape[0]
    offset = lax.axis_index("tp") * width_part
    local_taps = lax.dynamic_slice_in_dim(conv_taps, offset, width_part, 1)
    z_rows = (conv_input.astype(F32) * in_gate.astype(F32)).astype(BF)
    pairs = [(i, i + 1) for i in range(experts - 1)]
    rim = lax.ppermute(z_rows[:, length - (KERNEL - 1) :], ("z", "c"), pairs)
    longer = jnp.concatenate([rim, z_rows], axis=1).astype(F32)
    conv_sum = jnp.zeros(z_rows.shape, F32)
    for lag in range(KERNEL):
        begin = KERNEL - 1 - lag
        conv_sum = conv_sum + local_taps[lag][:, None] * longer[:, begin : begin + length]
    gated = (out_gate.astype(F32) * conv_sum).astype(BF)
    side = 4
    swap = [(0, 1), (1, 0)]
    place = lambda c, y, x: (c * side + y) * side + x
    span = range(side)
    along_x = lambda c: [[place(c, y, x) for x in span] for y in span]
    along_y = lambda c: [[place(c, y, x) for y in span] for x in span]
    early = along_x(0) + along_y(1)
    late = along_y(0) + along_x(1)

    def step(value, by, phase):
        pairs = []
        for c in range(2):
            for y in span:
                for x in span:
                    if (c == 0) == (phase == 0):
                        to = place(c, y, (x + by) % side)
                    else:
                        to = place(c, (y + by) % side, x)
                    pairs.append((place(c, y, x), to))
        return lax.ppermute(value, ("c", "tp"), pairs)

    gated = gated.reshape(2, width_part // 2, length)
    before = step(gated, 1, 0)
    after = step(gated, -1, 0)
    far = step(gated, 2, 0)
    line = jnp.concatenate([gated, after, far, before], axis=0)

    def exchange(value, groups):
        return lax.all_to_all(
            value, ("c", "tp"), 0, 0, axis_index_groups=groups, tiled=True
        )

    rows_own = arrived[:, 0].reshape(half, cols_part)
    rows_other = lax.ppermute(arrived[:, 1].reshape(half, cols_part), "c", swap)
    rows = jnp.concatenate([rows_own, rows_other], axis=0)
    quarter = exchange(jnp.broadcast_to(rows[None], (side,) + rows.shape), early)
    quarter, line = lax.optimization_barrier((quarter, line))
    x = exchange(jnp.broadcast_to(quarter[None], (side,) + quarter.shape), late)
    x = x.reshape(tp, slot_total, cols_part)
    weights = (expert_gate[0], expert_up[0], expert_down[0])
    part = expert_part(me, x, *weights, rows_b)
    part = part.reshape(side, side, slot_total, cols_part)
    half_sums = exchange(part, early).reshape(side, side * slot_total, cols_part)
    half_sums = sum_parts(half_sums, 8).reshape(side, slot_total, cols_part)
    half_sums, line = lax.optimization_barrier((half_sums, line))
    line_before = step(line, 1, 1)
    line_after = step(line, -1, 1)
    expert_rows = exchange(half_sums, late)
    expert_rows = sum_parts(expert_rows, 2)
    back_own = expert_rows[:half]
    back_other = lax.ppermute(expert_rows[half:], "c", swap)
    back = jnp.stack(
        [
            back_own.reshape(depth, capacity, cols_part),
            back_other.reshape(depth, capacity, cols_part),
        ],
        axis=1,
    )
    line_far_a = step(line_before[:4], 1, 1)
    line_far_b = step(line_after[4:], -1, 1)
    returned = lax.all_to_all(back, "z", 0, 0, tiled=True)
    blocks = mixer_proj.reshape(tp, width_part, cols_part)
    most = mixer_product(
        me, blocks, (line, line_after, line_before), (0, 1, 3), None, length // 4
    )
    mixed_out = mixer_product(
        me, blocks, (line_far_a, line_far_b), (2,), most, length // 4
    )
    returned, mixed_out = lax.optimization_barrier((returned, mixed_out))
    returned = returned.reshape(slot_total, cols_part)
    expert_out = pl.pallas_call(
        combine_kernel,
        out_shape=jax.ShapeDtypeStruct((rows_b, cols_part), BF),
        compiler_params=pltpu.CompilerParams(vmem_limit_bytes=12 * 1024 * 1024),
    )(places, route_weights, returned)
    return (mixed_out, expert_out)


def solution(mesh):
    ep, tp = mesh.devices.shape
    fine = Mesh(mesh.devices.reshape(ep // 2, 2, tp), ("z", "c", "tp"))
    both = ("z", "c")
    return jax.shard_map(
        layer,
        mesh=fine,
        in_specs=(
            P("tp", both),
            P("tp", both),
            P("tp", both),
            P(),
            P(None, "tp"),
            P(both, "tp"),
            P(both, None),
            P(both, None),
            P(both, None, "tp"),
            P(both, None, "tp"),
            P(both, "tp", None),
        ),
        out_specs=(P(both, "tp"), P(both, "tp")),
        check_vma=False,
    )
```

```python
import functools

import jax
import jax.numpy as jnp
from jax import lax
from jax.experimental import pallas as pl
from jax.experimental.pallas import tpu as pltpu
from jax.sharding import Mesh
from jax.sharding import PartitionSpec as P

KERNEL = 3
EPSILON = 1e-06
BF = jnp.bfloat16
F32 = jnp.float32


def ones_where(test):
    return jnp.where(test, 1.0, 0.0).astype(BF)


def dispatch_kernel(me_ref, routes_ref, rows_ref, places_ref, out_ref, *, experts, tp):
    core = me_ref[0] // tp
    rows = rows_ref.shape[0]
    slot_total = out_ref.shape[0]
    capacity = slot_total // experts
    ids = lax.broadcasted_iota(jnp.int32, (experts, rows), 0)
    named = [routes_ref[k : k + 1, :] for k in range(2)]
    hit = [n == ids for n in named]
    sooner = lax.broadcasted_iota(jnp.int32, (rows, rows), 0)
    later = lax.broadcasted_iota(jnp.int32, (rows, rows), 1)
    earlier = jnp.dot(
        ones_where(hit[0] | hit[1]), ones_where(sooner < later), preferred_element_type=F32
    )
    slots = lax.broadcasted_iota(jnp.int32, (slot_total, rows), 0)
    taken = []
    for k in range(2):
        slot = jnp.sum(jnp.where(hit[k], earlier, 0.0), axis=0, keepdims=True)
        place = (named[k] ^ core) * capacity + slot.astype(jnp.int32)
        places_ref[k : k + 1, :] = place
        taken.append(place == slots)
    out_ref[...] = jnp.dot(
        ones_where(taken[0] | taken[1]), rows_ref[...], preferred_element_type=F32
    ).astype(BF)


def combine_kernel(places_ref, weights_ref, own_ref, other_ref, out_ref, *, capacity):
    rows = out_ref.shape[0]
    slots = lax.broadcasted_iota(jnp.int32, (own_ref.shape[0], rows), 0)
    total = None
    for k in range(2):
        place = places_ref[k : k + 1, :]
        group = place // capacity
        within = (group // 2) * capacity + place % capacity
        match = within == slots
        picked = None
        for side, ref in enumerate((own_ref, other_ref)):
            part = lax.dot_general(
                ones_where(match & (group % 2 == side)),
                ref[...],
                (((0,), (0,)), ((), ())),
                preferred_element_type=F32,
            )
            picked = part if picked is None else picked + part
        term = picked * weights_ref[:, k : k + 1]
        total = term if total is None else total + term
    out_ref[...] = total.astype(BF)


def sum_kernel(in_ref, out_ref):
    total = in_ref[0].astype(F32)
    for j in range(1, in_ref.shape[0]):
        total = total + in_ref[j].astype(F32)
    out_ref[...] = total.astype(BF)


def expert_kernel(me_ref, x_ref, gate_ref, up_ref, down_ref, out_ref):
    parts = x_ref.shape[0]
    cols = x_ref.shape[2]
    side = 4
    core = me_ref[0] // parts
    natural = [j for j in range(parts)]
    turned = [(j % side) * side + j // side for j in range(parts)]
    load = [jnp.where(core == 0, natural[j], turned[j]) for j in range(parts)]
    store = [jnp.where(core == 0, turned[j], natural[j]) for j in range(parts)]
    x = jnp.concatenate([x_ref[load[j]] for j in range(parts)], axis=1)
    values = x.astype(F32)
    squares = jnp.sum(values * values, axis=1, keepdims=True)
    scale = lax.rsqrt(squares / (parts * cols) + EPSILON)
    gate = scale * jnp.dot(x, gate_ref[...], preferred_element_type=F32)
    up = scale * jnp.dot(x, up_ref[...], preferred_element_type=F32)
    hidden = (jax.nn.silu(gate) * up).astype(BF)
    part = jnp.dot(hidden, down_ref[...], preferred_element_type=F32).astype(BF)
    for j in range(parts):
        out_ref[store[j]] = part[:, j * cols : (j + 1) * cols]


def expert_part(me, x, gate_weight, up_weight, down_weight, tile):
    parts, rows, cols = x.shape
    whole = lambda w: pl.BlockSpec(w.shape, lambda i, c: (0, 0))
    return pl.pallas_call(
        expert_kernel,
        grid_spec=pltpu.PrefetchScalarGridSpec(
            num_scalar_prefetch=1,
            grid=(rows // tile,),
            in_specs=[
                pl.BlockSpec((parts, tile, cols), lambda i, c: (0, i, 0)),
                whole(gate_weight),
                whole(up_weight),
                whole(down_weight),
            ],
            out_specs=pl.BlockSpec((parts, tile, cols), lambda i, c: (0, i, 0)),
        ),
        out_shape=jax.ShapeDtypeStruct(x.shape, BF),
        compiler_params=pltpu.CompilerParams(vmem_limit_bytes=28 * 1024 * 1024),
        cost_estimate=pl.CostEstimate(
            flops=6 * rows * parts * cols * gate_weight.shape[1],
            bytes_accessed=2 * 2 * rows * parts * cols + 6 * gate_weight.size,
            transcendentals=rows * gate_weight.shape[1],
        ),
    )(me.reshape(1), x, gate_weight, up_weight, down_weight)


def mixer_kernel(me_ref, *refs, fars, last):
    refs, out_ref = refs[:-1], refs[-1]
    proj_ref, refs = refs[0], refs[1:]
    blocks = proj_ref.shape[0]
    side = 4
    core = me_ref[0] // blocks
    row = (me_ref[0] % blocks) // side
    col = me_ref[0] % side
    weights = []
    for far in fars:
        for near in range(side):
            down = jnp.where(core == 0, far, near)
            right = jnp.where(core == 0, near, far)
            at = ((row + down) % side) * side + (col + right) % side
            weights.append(proj_ref[at])
    proj = jnp.concatenate(weights, axis=0)
    pieces = refs[:-1] if last else refs
    y = jnp.concatenate([ref[i] for ref in pieces for i in range(ref.shape[0])], axis=0)
    flat = lax.dot_general(
        proj, y, (((0,), (0,)), ((), ())), preferred_element_type=F32
    )
    if last:
        out_ref[...] = jnp.transpose(flat + refs[-1][...]).astype(BF)
    else:
        out_ref[...] = flat


def mixer_product(me, proj, pieces, fars, base, tile):
    length = pieces[0].shape[2]
    _, width, cols = proj.shape
    last = base is not None
    flat_spec = pl.BlockSpec((cols, tile), lambda i, c: (0, i))
    return pl.pallas_call(
        functools.partial(mixer_kernel, fars=fars, last=last),
        grid_spec=pltpu.PrefetchScalarGridSpec(
            num_scalar_prefetch=1,
            grid=(length // tile,),
            in_specs=[pl.BlockSpec(proj.shape, lambda i, c: (0, 0, 0))]
            + [
                pl.BlockSpec(p.shape[:2] + (tile,), lambda i, c: (0, 0, i)) for p in pieces
            ]
            + ([flat_spec] if last else []),
            out_specs=pl.BlockSpec((tile, cols), lambda i, c: (i, 0)) if last else flat_spec,
        ),
        out_shape=jax.ShapeDtypeStruct((length, cols), BF)
        if last
        else jax.ShapeDtypeStruct((cols, length), F32),
        compiler_params=pltpu.CompilerParams(vmem_limit_bytes=16 * 1024 * 1024),
        cost_estimate=pl.CostEstimate(
            flops=2 * length * len(fars) * 4 * width * cols,
            bytes_accessed=2 * length * (len(fars) * 4 * width + 2 * cols) + 2 * proj.size,
            transcendentals=0,
        ),
    )(me.reshape(1), proj, *pieces, *([base] if last else []))


def sum_parts(arrived, steps):
    parts, rows, cols = arrived.shape
    return pl.pallas_call(
        sum_kernel,
        grid=(steps,),
        in_specs=[pl.BlockSpec((parts, rows // steps, cols), lambda i: (0, i, 0))],
        out_specs=pl.BlockSpec((rows // steps, cols), lambda i: (i, 0)),
        out_shape=jax.ShapeDtypeStruct((rows, cols), BF),
        compiler_params=pltpu.CompilerParams(vmem_limit_bytes=12 * 1024 * 1024),
    )(arrived)


def layer(
    conv_input,
    out_gate,
    in_gate,
    conv_taps,
    mixer_proj,
    token_rows,
    routes,
    route_weights,
    expert_gate,
    expert_up,
    expert_down,
):
    depth = lax.axis_size("z")
    experts = 2 * depth
    tp = lax.axis_size("tp")
    me = lax.axis_index(("c", "tp"))
    rows_b, cols_part = token_rows.shape
    capacity = 4 * rows_b // experts
    slot_total = experts * capacity
    half = slot_total // 2

    by_choice = routes.T
    places, outgoing = pl.pallas_call(
        functools.partial(dispatch_kernel, experts=experts, tp=tp),
        grid_spec=pltpu.PrefetchScalarGridSpec(
            num_scalar_prefetch=1,
            grid=(1,),
            in_specs=[
                pl.BlockSpec(by_choice.shape, lambda i, c: (0, 0)),
                pl.BlockSpec(token_rows.shape, lambda i, c: (0, 0)),
            ],
            out_specs=[
                pl.BlockSpec(by_choice.shape, lambda i, c: (0, 0)),
                pl.BlockSpec((slot_total, cols_part), lambda i, c: (0, 0)),
            ],
        ),
        out_shape=[
            jax.ShapeDtypeStruct(by_choice.shape, jnp.int32),
            jax.ShapeDtypeStruct((slot_total, cols_part), BF),
        ],
        compiler_params=pltpu.CompilerParams(vmem_limit_bytes=12 * 1024 * 1024),
    )(me.reshape(1), by_choice, token_rows)
    outgoing, conv_input, in_gate = lax.optimization_barrier((outgoing, conv_input, in_gate))
    arrived = lax.all_to_all(
        outgoing.reshape(depth, 2, capacity, cols_part), "z", 0, 0, tiled=True
    )

    length = conv_input.shape[1]
    width_part = conv_input.shape[0]
    offset = lax.axis_index("tp") * width_part
    local_taps = lax.dynamic_slice_in_dim(conv_taps, offset, width_part, 1)
    z_rows = (conv_input.astype(F32) * in_gate.astype(F32)).astype(BF)
    pairs = [(i, i + 1) for i in range(experts - 1)]
    rim = lax.ppermute(z_rows[:, length - (KERNEL - 1) :], ("z", "c"), pairs)
    longer = jnp.concatenate([rim, z_rows], axis=1).astype(F32)
    conv_sum = jnp.zeros(z_rows.shape, F32)
    for lag in range(KERNEL):
        begin = KERNEL - 1 - lag
        conv_sum = conv_sum + local_taps[lag][:, None] * longer[:, begin : begin + length]
    gated = (out_gate.astype(F32) * conv_sum).astype(BF)
    side = 4
    swap = [(0, 1), (1, 0)]
    place = lambda c, y, x: (c * side + y) * side + x
    span = range(side)
    along_x = lambda c: [[place(c, y, x) for x in span] for y in span]
    along_y = lambda c: [[place(c, y, x) for y in span] for x in span]
    early = along_x(0) + along_y(1)
    late = along_y(0) + along_x(1)

    def step(value, by, phase):
        pairs = []
        for c in range(2):
            for y in span:
                for x in span:
                    if (c == 0) == (phase == 0):
                        to = place(c, y, (x + by) % side)
                    else:
                        to = place(c, (y + by) % side, x)
                    pairs.append((place(c, y, x), to))
        return lax.ppermute(value, ("c", "tp"), pairs)

    gated = gated.reshape(2, width_part // 2, length)
    before = step(gated, 1, 0)
    after = step(gated, -1, 0)
    far = step(gated, 2, 0)
    line = jnp.concatenate([gated, after, far, before], axis=0)

    def exchange(value, groups):
        return lax.all_to_all(
            value, ("c", "tp"), 0, 0, axis_index_groups=groups, tiled=True
        )

    rows_other = lax.ppermute(arrived[:, 1], "c", swap)
    rows = jnp.stack([arrived[:, 0], rows_other], axis=1).reshape(slot_total, cols_part)
    quarter = exchange(jnp.broadcast_to(rows[None], (side,) + rows.shape), early)
    quarter, line = lax.optimization_barrier((quarter, line))
    x = exchange(jnp.broadcast_to(quarter[None], (side,) + quarter.shape), late)
    x = x.reshape(tp, slot_total, cols_part)
    weights = (expert_gate[0], expert_up[0], expert_down[0])
    part = expert_part(me, x, *weights, rows_b)
    part = part.reshape(side, side, slot_total, cols_part)
    half_sums = exchange(part, early).reshape(side, side * slot_total, cols_part)
    half_sums = sum_parts(half_sums, 8).reshape(side, slot_total, cols_part)
    half_sums, line = lax.optimization_barrier((half_sums, line))
    line_before = step(line, 1, 1)
    line_after = step(line, -1, 1)
    line_far = step(line, 2, 1)
    expert_rows = exchange(half_sums, late)
    expert_rows = sum_parts(expert_rows, 2)
    back = expert_rows.reshape(depth, 2, capacity, cols_part)
    returned = lax.all_to_all(back, "z", 0, 0, tiled=True)
    blocks = mixer_proj.reshape(tp, width_part, cols_part)
    most = mixer_product(
        me, blocks, (line, line_after, line_before), (0, 1, 3), None, length // 4
    )
    returned, most = lax.optimization_barrier((returned, most))
    returned_own = returned[:, 0].reshape(half, cols_part)
    returned_other = lax.ppermute(returned[:, 1].reshape(half, cols_part), "c", swap)
    mixed_out = mixer_product(
        me, blocks, (line_far,), (2,), most, length // 4
    )
    returned_other, mixed_out = lax.optimization_barrier((returned_other, mixed_out))
    expert_out = pl.pallas_call(
        functools.partial(combine_kernel, capacity=capacity),
        out_shape=jax.ShapeDtypeStruct((rows_b, cols_part), BF),
        compiler_params=pltpu.CompilerParams(vmem_limit_bytes=12 * 1024 * 1024),
    )(places, route_weights, returned_own, returned_other)
    return (mixed_out, expert_out)


def solution(mesh):
    ep, tp = mesh.devices.shape
    fine = Mesh(mesh.devices.reshape(ep // 2, 2, tp), ("z", "c", "tp"))
    both = ("z", "c")
    return jax.shard_map(
        layer,
        mesh=fine,
        in_specs=(
            P("tp", both),
            P("tp", both),
            P("tp", both),
            P(),
            P(None, "tp"),
            P(both, "tp"),
            P(both, None),
            P(both, None),
            P(both, None, "tp"),
            P(both, None, "tp"),
            P(both, "tp", None),
        ),
        out_specs=(P(both, "tp"), P(both, "tp")),
        check_vma=False,
    )
```

```python
import functools

import jax
import jax.numpy as jnp
from jax import lax
from jax.experimental import pallas as pl
from jax.experimental.pallas import tpu as pltpu
from jax.sharding import Mesh
from jax.sharding import PartitionSpec as P

KERNEL = 3
EPSILON = 1e-06
BF = jnp.bfloat16
F32 = jnp.float32


def ones_where(test):
    return jnp.where(test, 1.0, 0.0).astype(BF)


def dispatch_kernel(me_ref, routes_ref, rows_ref, places_ref, out_ref, *, experts, tp):
    core = me_ref[0] // tp
    rows = rows_ref.shape[0]
    slot_total = out_ref.shape[0]
    capacity = slot_total // experts
    ids = lax.broadcasted_iota(jnp.int32, (experts, rows), 0)
    named = [routes_ref[k : k + 1, :] for k in range(2)]
    hit = [n == ids for n in named]
    sooner = lax.broadcasted_iota(jnp.int32, (rows, rows), 0)
    later = lax.broadcasted_iota(jnp.int32, (rows, rows), 1)
    earlier = jnp.dot(
        ones_where(hit[0] | hit[1]), ones_where(sooner < later), preferred_element_type=F32
    )
    slots = lax.broadcasted_iota(jnp.int32, (slot_total, rows), 0)
    taken = []
    for k in range(2):
        slot = jnp.sum(jnp.where(hit[k], earlier, 0.0), axis=0, keepdims=True)
        place = (named[k] ^ core) * capacity + slot.astype(jnp.int32)
        places_ref[k : k + 1, :] = place
        taken.append(place == slots)
    out_ref[...] = jnp.dot(
        ones_where(taken[0] | taken[1]), rows_ref[...], preferred_element_type=F32
    ).astype(BF)


def combine_kernel(places_ref, weights_ref, own_ref, other_ref, out_ref, *, capacity):
    rows = out_ref.shape[0]
    slots = lax.broadcasted_iota(jnp.int32, (own_ref.shape[0], rows), 0)
    total = None
    for k in range(2):
        place = places_ref[k : k + 1, :]
        group = place // capacity
        within = (group // 2) * capacity + place % capacity
        match = within == slots
        picked = None
        for side, ref in enumerate((own_ref, other_ref)):
            part = lax.dot_general(
                ones_where(match & (group % 2 == side)),
                ref[...],
                (((0,), (0,)), ((), ())),
                preferred_element_type=F32,
            )
            picked = part if picked is None else picked + part
        term = picked * weights_ref[:, k : k + 1]
        total = term if total is None else total + term
    out_ref[...] = total.astype(BF)


def sum_kernel(in_ref, out_ref):
    total = in_ref[0].astype(F32)
    for j in range(1, in_ref.shape[0]):
        total = total + in_ref[j].astype(F32)
    out_ref[...] = total.astype(BF)


def expert_kernel(me_ref, x_ref, gate_ref, up_ref, down_ref, out_ref):
    parts = x_ref.shape[0]
    cols = x_ref.shape[2]
    side = 4
    core = me_ref[0] // parts
    natural = [j for j in range(parts)]
    turned = [(j % side) * side + j // side for j in range(parts)]
    load = [jnp.where(core == 0, natural[j], turned[j]) for j in range(parts)]
    store = [jnp.where(core == 0, turned[j], natural[j]) for j in range(parts)]
    x = jnp.concatenate([x_ref[load[j]] for j in range(parts)], axis=1)
    values = x.astype(F32)
    squares = jnp.sum(values * values, axis=1, keepdims=True)
    scale = lax.rsqrt(squares / (parts * cols) + EPSILON)
    gate = scale * jnp.dot(x, gate_ref[...], preferred_element_type=F32)
    up = scale * jnp.dot(x, up_ref[...], preferred_element_type=F32)
    hidden = (jax.nn.silu(gate) * up).astype(BF)
    part = jnp.dot(hidden, down_ref[...], preferred_element_type=F32).astype(BF)
    for j in range(parts):
        out_ref[store[j]] = part[:, j * cols : (j + 1) * cols]


def expert_part(me, x, gate_weight, up_weight, down_weight, tile):
    parts, rows, cols = x.shape
    whole = lambda w: pl.BlockSpec(w.shape, lambda i, c: (0, 0))
    return pl.pallas_call(
        expert_kernel,
        grid_spec=pltpu.PrefetchScalarGridSpec(
            num_scalar_prefetch=1,
            grid=(rows // tile,),
            in_specs=[
                pl.BlockSpec((parts, tile, cols), lambda i, c: (0, i, 0)),
                whole(gate_weight),
                whole(up_weight),
                whole(down_weight),
            ],
            out_specs=pl.BlockSpec((parts, tile, cols), lambda i, c: (0, i, 0)),
        ),
        out_shape=jax.ShapeDtypeStruct(x.shape, BF),
        compiler_params=pltpu.CompilerParams(vmem_limit_bytes=28 * 1024 * 1024),
        cost_estimate=pl.CostEstimate(
            flops=6 * rows * parts * cols * gate_weight.shape[1],
            bytes_accessed=2 * 2 * rows * parts * cols + 6 * gate_weight.size,
            transcendentals=rows * gate_weight.shape[1],
        ),
    )(me.reshape(1), x, gate_weight, up_weight, down_weight)


def mixer_kernel(me_ref, *refs, fars, last):
    refs, out_ref = refs[:-1], refs[-1]
    proj_ref, refs = refs[0], refs[1:]
    blocks = proj_ref.shape[0]
    side = 4
    core = me_ref[0] // blocks
    row = (me_ref[0] % blocks) // side
    col = me_ref[0] % side
    weights = []
    for far in fars:
        for near in range(side):
            down = jnp.where(core == 0, far, near)
            right = jnp.where(core == 0, near, far)
            at = ((row + down) % side) * side + (col + right) % side
            weights.append(proj_ref[at])
    proj = jnp.concatenate(weights, axis=0)
    pieces = refs[:-1] if last else refs
    y = jnp.concatenate([ref[i] for ref in pieces for i in range(ref.shape[0])], axis=0)
    flat = lax.dot_general(
        proj, y, (((0,), (0,)), ((), ())), preferred_element_type=F32
    )
    if last:
        out_ref[...] = jnp.transpose(flat + refs[-1][...]).astype(BF)
    else:
        out_ref[...] = flat


def mixer_product(me, proj, pieces, fars, base, tile):
    length = pieces[0].shape[2]
    _, width, cols = proj.shape
    last = base is not None
    flat_spec = pl.BlockSpec((cols, tile), lambda i, c: (0, i))
    return pl.pallas_call(
        functools.partial(mixer_kernel, fars=fars, last=last),
        grid_spec=pltpu.PrefetchScalarGridSpec(
            num_scalar_prefetch=1,
            grid=(length // tile,),
            in_specs=[pl.BlockSpec(proj.shape, lambda i, c: (0, 0, 0))]
            + [
                pl.BlockSpec(p.shape[:2] + (tile,), lambda i, c: (0, 0, i)) for p in pieces
            ]
            + ([flat_spec] if last else []),
            out_specs=pl.BlockSpec((tile, cols), lambda i, c: (i, 0)) if last else flat_spec,
        ),
        out_shape=jax.ShapeDtypeStruct((length, cols), BF)
        if last
        else jax.ShapeDtypeStruct((cols, length), F32),
        compiler_params=pltpu.CompilerParams(vmem_limit_bytes=16 * 1024 * 1024),
        cost_estimate=pl.CostEstimate(
            flops=2 * length * len(fars) * 4 * width * cols,
            bytes_accessed=2 * length * (len(fars) * 4 * width + 2 * cols) + 2 * proj.size,
            transcendentals=0,
        ),
    )(me.reshape(1), proj, *pieces, *([base] if last else []))


def sum_parts(arrived, steps):
    parts, rows, cols = arrived.shape
    return pl.pallas_call(
        sum_kernel,
        grid=(steps,),
        in_specs=[pl.BlockSpec((parts, rows // steps, cols), lambda i: (0, i, 0))],
        out_specs=pl.BlockSpec((rows // steps, cols), lambda i: (i, 0)),
        out_shape=jax.ShapeDtypeStruct((rows, cols), BF),
        compiler_params=pltpu.CompilerParams(vmem_limit_bytes=12 * 1024 * 1024),
    )(arrived)


def layer(
    conv_input,
    out_gate,
    in_gate,
    conv_taps,
    mixer_proj,
    token_rows,
    routes,
    route_weights,
    expert_gate,
    expert_up,
    expert_down,
):
    depth = lax.axis_size("z")
    experts = 2 * depth
    tp = lax.axis_size("tp")
    me = lax.axis_index(("c", "tp"))
    rows_b, cols_part = token_rows.shape
    capacity = 4 * rows_b // experts
    slot_total = experts * capacity
    half = slot_total // 2

    by_choice = routes.T
    places, outgoing = pl.pallas_call(
        functools.partial(dispatch_kernel, experts=experts, tp=tp),
        grid_spec=pltpu.PrefetchScalarGridSpec(
            num_scalar_prefetch=1,
            grid=(1,),
            in_specs=[
                pl.BlockSpec(by_choice.shape, lambda i, c: (0, 0)),
                pl.BlockSpec(token_rows.shape, lambda i, c: (0, 0)),
            ],
            out_specs=[
                pl.BlockSpec(by_choice.shape, lambda i, c: (0, 0)),
                pl.BlockSpec((slot_total, cols_part), lambda i, c: (0, 0)),
            ],
        ),
        out_shape=[
            jax.ShapeDtypeStruct(by_choice.shape, jnp.int32),
            jax.ShapeDtypeStruct((slot_total, cols_part), BF),
        ],
        compiler_params=pltpu.CompilerParams(vmem_limit_bytes=12 * 1024 * 1024),
    )(me.reshape(1), by_choice, token_rows)
    outgoing, conv_input, in_gate = lax.optimization_barrier((outgoing, conv_input, in_gate))
    arrived = lax.all_to_all(
        outgoing.reshape(depth, 2, capacity, cols_part), "z", 0, 0, tiled=True
    )

    length = conv_input.shape[1]
    width_part = conv_input.shape[0]
    offset = lax.axis_index("tp") * width_part
    local_taps = lax.dynamic_slice_in_dim(conv_taps, offset, width_part, 1)
    z_rows = (conv_input.astype(F32) * in_gate.astype(F32)).astype(BF)
    pairs = [(i, i + 1) for i in range(experts - 1)]
    rim = lax.ppermute(z_rows[:, length - (KERNEL - 1) :], ("z", "c"), pairs)
    longer = jnp.concatenate([rim, z_rows], axis=1).astype(F32)
    conv_sum = jnp.zeros(z_rows.shape, F32)
    for lag in range(KERNEL):
        begin = KERNEL - 1 - lag
        conv_sum = conv_sum + local_taps[lag][:, None] * longer[:, begin : begin + length]
    gated = (out_gate.astype(F32) * conv_sum).astype(BF)
    side = 4
    swap = [(0, 1), (1, 0)]
    place = lambda c, y, x: (c * side + y) * side + x
    span = range(side)
    along_x = lambda c: [[place(c, y, x) for x in span] for y in span]
    along_y = lambda c: [[place(c, y, x) for y in span] for x in span]
    early = along_x(0) + along_y(1)
    late = along_y(0) + along_x(1)

    def step(value, by, phase):
        pairs = []
        for c in range(2):
            for y in span:
                for x in span:
                    if (c == 0) == (phase == 0):
                        to = place(c, y, (x + by) % side)
                    else:
                        to = place(c, (y + by) % side, x)
                    pairs.append((place(c, y, x), to))
        return lax.ppermute(value, ("c", "tp"), pairs)

    gated = gated.reshape(2, width_part // 2, length)
    before = step(gated, 1, 0)
    after = step(gated, -1, 0)
    far = step(gated, 2, 0)
    line = jnp.concatenate([gated, after, far, before], axis=0)

    def exchange(value, groups):
        return lax.all_to_all(
            value, ("c", "tp"), 0, 0, axis_index_groups=groups, tiled=True
        )

    rows_other = lax.ppermute(arrived[:, 1], "c", swap)
    rows = jnp.stack([arrived[:, 0], rows_other], axis=1).reshape(slot_total, cols_part)
    quarter = exchange(jnp.broadcast_to(rows[None], (side,) + rows.shape), early)
    quarter, line = lax.optimization_barrier((quarter, line))
    x = exchange(jnp.broadcast_to(quarter[None], (side,) + quarter.shape), late)
    x = x.reshape(tp, slot_total, cols_part)
    weights = (expert_gate[0], expert_up[0], expert_down[0])
    part = expert_part(me, x, *weights, rows_b)
    part = part.reshape(side, side, slot_total, cols_part)
    half_sums = exchange(part, early).reshape(side, side * slot_total, cols_part)
    half_sums = sum_parts(half_sums, 4).reshape(side, slot_total, cols_part)
    half_sums, line = lax.optimization_barrier((half_sums, line))
    line_before = step(line, 1, 1)
    line_after = step(line, -1, 1)
    expert_rows = exchange(half_sums, late)
    expert_rows = sum_parts(expert_rows, 2)
    back = expert_rows.reshape(depth, 2, capacity, cols_part)
    line_far_a = step(line_before[:4], 1, 1)
    line_far_b = step(line_after[4:], -1, 1)
    returned = lax.all_to_all(back, "z", 0, 0, tiled=True)
    blocks = mixer_proj.reshape(tp, width_part, cols_part)
    most = mixer_product(
        me, blocks, (line, line_after, line_before), (0, 1, 3), None, length // 4
    )
    returned, most = lax.optimization_barrier((returned, most))
    returned_own = returned[:, 0].reshape(half, cols_part)
    returned_other = lax.ppermute(returned[:, 1].reshape(half, cols_part), "c", swap)
    mixed_out = mixer_product(
        me, blocks, (line_far_a, line_far_b), (2,), most, length // 2
    )
    returned_other, mixed_out = lax.optimization_barrier((returned_other, mixed_out))
    expert_out = pl.pallas_call(
        functools.partial(combine_kernel, capacity=capacity),
        out_shape=jax.ShapeDtypeStruct((rows_b, cols_part), BF),
        compiler_params=pltpu.CompilerParams(vmem_limit_bytes=12 * 1024 * 1024),
    )(places, route_weights, returned_own, returned_other)
    return (mixed_out, expert_out)


def solution(mesh):
    ep, tp = mesh.devices.shape
    fine = Mesh(mesh.devices.reshape(ep // 2, 2, tp), ("z", "c", "tp"))
    both = ("z", "c")
    return jax.shard_map(
        layer,
        mesh=fine,
        in_specs=(
            P("tp", both),
            P("tp", both),
            P("tp", both),
            P(),
            P(None, "tp"),
            P(both, "tp"),
            P(both, None),
            P(both, None),
            P(both, None, "tp"),
            P(both, None, "tp"),
            P(both, "tp", None),
        ),
        out_specs=(P(both, "tp"), P(both, "tp")),
        check_vma=False,
    )
```

```python
import functools

import jax
import jax.numpy as jnp
from jax import lax
from jax.experimental import pallas as pl
from jax.experimental.pallas import tpu as pltpu
from jax.sharding import Mesh
from jax.sharding import PartitionSpec as P

KERNEL = 3
EPSILON = 1e-06
BF = jnp.bfloat16
F32 = jnp.float32


def ones_where(test):
    return jnp.where(test, 1.0, 0.0).astype(BF)


def dispatch_kernel(me_ref, routes_ref, rows_ref, places_ref, out_ref, *, experts, tp):
    core = me_ref[0] // tp
    rows = rows_ref.shape[0]
    slot_total = out_ref.shape[0]
    capacity = slot_total // experts
    ids = lax.broadcasted_iota(jnp.int32, (experts, rows), 0)
    named = [routes_ref[k : k + 1, :] for k in range(2)]
    hit = [n == ids for n in named]
    sooner = lax.broadcasted_iota(jnp.int32, (rows, rows), 0)
    later = lax.broadcasted_iota(jnp.int32, (rows, rows), 1)
    earlier = jnp.dot(
        ones_where(hit[0] | hit[1]), ones_where(sooner < later), preferred_element_type=F32
    )
    slots = lax.broadcasted_iota(jnp.int32, (slot_total, rows), 0)
    taken = []
    for k in range(2):
        slot = jnp.sum(jnp.where(hit[k], earlier, 0.0), axis=0, keepdims=True)
        place = (named[k] ^ core) * capacity + slot.astype(jnp.int32)
        places_ref[k : k + 1, :] = place
        taken.append(place == slots)
    out_ref[...] = jnp.dot(
        ones_where(taken[0] | taken[1]), rows_ref[...], preferred_element_type=F32
    ).astype(BF)


def combine_kernel(places_ref, weights_ref, own_ref, other_ref, out_ref, *, capacity):
    rows = out_ref.shape[0]
    slots = lax.broadcasted_iota(jnp.int32, (own_ref.shape[0], rows), 0)
    total = None
    for k in range(2):
        place = places_ref[k : k + 1, :]
        group = place // capacity
        within = (group // 2) * capacity + place % capacity
        match = within == slots
        picked = None
        for side, ref in enumerate((own_ref, other_ref)):
            part = lax.dot_general(
                ones_where(match & (group % 2 == side)),
                ref[...],
                (((0,), (0,)), ((), ())),
                preferred_element_type=F32,
            )
            picked = part if picked is None else picked + part
        term = picked * weights_ref[:, k : k + 1]
        total = term if total is None else total + term
    out_ref[...] = total.astype(BF)


def sum_kernel(in_ref, out_ref):
    total = in_ref[0].astype(F32)
    for j in range(1, in_ref.shape[0]):
        total = total + in_ref[j].astype(F32)
    out_ref[...] = total.astype(BF)


def expert_kernel(me_ref, x_ref, gate_ref, up_ref, down_ref, out_ref):
    parts = x_ref.shape[0]
    cols = x_ref.shape[2]
    side = 4
    core = me_ref[0] // parts
    natural = [j for j in range(parts)]
    turned = [(j % side) * side + j // side for j in range(parts)]
    load = [jnp.where(core == 0, natural[j], turned[j]) for j in range(parts)]
    store = [jnp.where(core == 0, turned[j], natural[j]) for j in range(parts)]
    x = jnp.concatenate([x_ref[load[j]] for j in range(parts)], axis=1)
    values = x.astype(F32)
    squares = jnp.sum(values * values, axis=1, keepdims=True)
    scale = lax.rsqrt(squares / (parts * cols) + EPSILON)
    gate = scale * jnp.dot(x, gate_ref[...], preferred_element_type=F32)
    up = scale * jnp.dot(x, up_ref[...], preferred_element_type=F32)
    hidden = (jax.nn.silu(gate) * up).astype(BF)
    part = jnp.dot(hidden, down_ref[...], preferred_element_type=F32).astype(BF)
    for j in range(parts):
        out_ref[store[j]] = part[:, j * cols : (j + 1) * cols]


def expert_part(me, x, gate_weight, up_weight, down_weight, tile):
    parts, rows, cols = x.shape
    whole = lambda w: pl.BlockSpec(w.shape, lambda i, c: (0, 0))
    return pl.pallas_call(
        expert_kernel,
        grid_spec=pltpu.PrefetchScalarGridSpec(
            num_scalar_prefetch=1,
            grid=(rows // tile,),
            in_specs=[
                pl.BlockSpec((parts, tile, cols), lambda i, c: (0, i, 0)),
                whole(gate_weight),
                whole(up_weight),
                whole(down_weight),
            ],
            out_specs=pl.BlockSpec((parts, tile, cols), lambda i, c: (0, i, 0)),
        ),
        out_shape=jax.ShapeDtypeStruct(x.shape, BF),
        compiler_params=pltpu.CompilerParams(vmem_limit_bytes=28 * 1024 * 1024),
        cost_estimate=pl.CostEstimate(
            flops=6 * rows * parts * cols * gate_weight.shape[1],
            bytes_accessed=2 * 2 * rows * parts * cols + 6 * gate_weight.size,
            transcendentals=rows * gate_weight.shape[1],
        ),
    )(me.reshape(1), x, gate_weight, up_weight, down_weight)


def mixer_kernel(me_ref, *refs, fars, last):
    refs, out_ref = refs[:-1], refs[-1]
    proj_ref, refs = refs[0], refs[1:]
    blocks = proj_ref.shape[0]
    side = 4
    core = me_ref[0] // blocks
    row = (me_ref[0] % blocks) // side
    col = me_ref[0] % side
    weights = []
    for far in fars:
        for near in range(side):
            down = jnp.where(core == 0, far, near)
            right = jnp.where(core == 0, near, far)
            at = ((row + down) % side) * side + (col + right) % side
            weights.append(proj_ref[at])
    proj = jnp.concatenate(weights, axis=0)
    pieces = refs[:-1] if last else refs
    y = jnp.concatenate([ref[i] for ref in pieces for i in range(ref.shape[0])], axis=0)
    flat = lax.dot_general(
        proj, y, (((0,), (0,)), ((), ())), preferred_element_type=F32
    )
    if last:
        out_ref[...] = jnp.transpose(flat + refs[-1][...]).astype(BF)
    else:
        out_ref[...] = flat


def mixer_product(me, proj, pieces, fars, base, tile):
    length = pieces[0].shape[2]
    _, width, cols = proj.shape
    last = base is not None
    flat_spec = pl.BlockSpec((cols, tile), lambda i, c: (0, i))
    return pl.pallas_call(
        functools.partial(mixer_kernel, fars=fars, last=last),
        grid_spec=pltpu.PrefetchScalarGridSpec(
            num_scalar_prefetch=1,
            grid=(length // tile,),
            in_specs=[pl.BlockSpec(proj.shape, lambda i, c: (0, 0, 0))]
            + [
                pl.BlockSpec(p.shape[:2] + (tile,), lambda i, c: (0, 0, i)) for p in pieces
            ]
            + ([flat_spec] if last else []),
            out_specs=pl.BlockSpec((tile, cols), lambda i, c: (i, 0)) if last else flat_spec,
        ),
        out_shape=jax.ShapeDtypeStruct((length, cols), BF)
        if last
        else jax.ShapeDtypeStruct((cols, length), F32),
        compiler_params=pltpu.CompilerParams(vmem_limit_bytes=16 * 1024 * 1024),
        cost_estimate=pl.CostEstimate(
            flops=2 * length * len(fars) * 4 * width * cols,
            bytes_accessed=2 * length * (len(fars) * 4 * width + 2 * cols) + 2 * proj.size,
            transcendentals=0,
        ),
    )(me.reshape(1), proj, *pieces, *([base] if last else []))


def sum_parts(arrived, steps):
    parts, rows, cols = arrived.shape
    return pl.pallas_call(
        sum_kernel,
        grid=(steps,),
        in_specs=[pl.BlockSpec((parts, rows // steps, cols), lambda i: (0, i, 0))],
        out_specs=pl.BlockSpec((rows // steps, cols), lambda i: (i, 0)),
        out_shape=jax.ShapeDtypeStruct((rows, cols), BF),
        compiler_params=pltpu.CompilerParams(vmem_limit_bytes=12 * 1024 * 1024),
    )(arrived)


def layer(
    conv_input,
    out_gate,
    in_gate,
    conv_taps,
    mixer_proj,
    token_rows,
    routes,
    route_weights,
    expert_gate,
    expert_up,
    expert_down,
):
    depth = lax.axis_size("z")
    experts = 2 * depth
    tp = lax.axis_size("tp")
    me = lax.axis_index(("c", "tp"))
    rows_b, cols_part = token_rows.shape
    capacity = 4 * rows_b // experts
    slot_total = experts * capacity
    half = slot_total // 2

    by_choice = routes.T
    places, outgoing = pl.pallas_call(
        functools.partial(dispatch_kernel, experts=experts, tp=tp),
        grid_spec=pltpu.PrefetchScalarGridSpec(
            num_scalar_prefetch=1,
            grid=(1,),
            in_specs=[
                pl.BlockSpec(by_choice.shape, lambda i, c: (0, 0)),
                pl.BlockSpec(token_rows.shape, lambda i, c: (0, 0)),
            ],
            out_specs=[
                pl.BlockSpec(by_choice.shape, lambda i, c: (0, 0)),
                pl.BlockSpec((slot_total, cols_part), lambda i, c: (0, 0)),
            ],
        ),
        out_shape=[
            jax.ShapeDtypeStruct(by_choice.shape, jnp.int32),
            jax.ShapeDtypeStruct((slot_total, cols_part), BF),
        ],
        compiler_params=pltpu.CompilerParams(vmem_limit_bytes=12 * 1024 * 1024),
    )(me.reshape(1), by_choice, token_rows)
    outgoing, conv_input, in_gate = lax.optimization_barrier((outgoing, conv_input, in_gate))
    arrived = lax.all_to_all(
        outgoing.reshape(depth, 2, capacity, cols_part), "z", 0, 0, tiled=True
    )

    length = conv_input.shape[1]
    width_part = conv_input.shape[0]
    offset = lax.axis_index("tp") * width_part
    local_taps = lax.dynamic_slice_in_dim(conv_taps, offset, width_part, 1)
    z_rows = (conv_input.astype(F32) * in_gate.astype(F32)).astype(BF)
    pairs = [(i, i + 1) for i in range(experts - 1)]
    rim = lax.ppermute(z_rows[:, length - (KERNEL - 1) :], ("z", "c"), pairs)
    longer = jnp.concatenate([rim, z_rows], axis=1).astype(F32)
    conv_sum = jnp.zeros(z_rows.shape, F32)
    for lag in range(KERNEL):
        begin = KERNEL - 1 - lag
        conv_sum = conv_sum + local_taps[lag][:, None] * longer[:, begin : begin + length]
    gated = (out_gate.astype(F32) * conv_sum).astype(BF)
    side = 4
    swap = [(0, 1), (1, 0)]
    place = lambda c, y, x: (c * side + y) * side + x
    span = range(side)
    along_x = lambda c: [[place(c, y, x) for x in span] for y in span]
    along_y = lambda c: [[place(c, y, x) for y in span] for x in span]
    early = along_x(0) + along_y(1)
    late = along_y(0) + along_x(1)

    def step(value, by, phase):
        pairs = []
        for c in range(2):
            for y in span:
                for x in span:
                    if (c == 0) == (phase == 0):
                        to = place(c, y, (x + by) % side)
                    else:
                        to = place(c, (y + by) % side, x)
                    pairs.append((place(c, y, x), to))
        return lax.ppermute(value, ("c", "tp"), pairs)

    gated = gated.reshape(2, width_part // 2, length)
    before = step(gated, 1, 0)
    after = step(gated, -1, 0)
    far = step(gated, 2, 0)
    line = jnp.concatenate([gated, after, far, before], axis=0)

    def exchange(value, groups):
        return lax.all_to_all(
            value, ("c", "tp"), 0, 0, axis_index_groups=groups, tiled=True
        )

    rows_other = lax.ppermute(arrived[:, 1], "c", swap)
    rows = jnp.stack([arrived[:, 0], rows_other], axis=1).reshape(slot_total, cols_part)
    quarter = exchange(jnp.broadcast_to(rows[None], (side,) + rows.shape), early)
    quarter, line = lax.optimization_barrier((quarter, line))
    x = exchange(jnp.broadcast_to(quarter[None], (side,) + quarter.shape), late)
    x = x.reshape(tp, slot_total, cols_part)
    weights = (expert_gate[0], expert_up[0], expert_down[0])
    part = expert_part(me, x, *weights, rows_b)
    part = part.reshape(side, side, slot_total, cols_part)
    half_sums = exchange(part, early).reshape(side, side * slot_total, cols_part)
    half_sums = sum_parts(half_sums, 2).reshape(side, slot_total, cols_part)
    half_sums, line = lax.optimization_barrier((half_sums, line))
    line_before = step(line, 1, 1)
    line_after = step(line, -1, 1)
    expert_rows = exchange(half_sums, late)
    expert_rows = sum_parts(expert_rows, 2)
    back = expert_rows.reshape(depth, 2, capacity, cols_part)
    line_far_a = step(line_before[:4], 1, 1)
    line_far_b = step(line_after[4:], -1, 1)
    returned = lax.all_to_all(back, "z", 0, 0, tiled=True)
    blocks = mixer_proj.reshape(tp, width_part, cols_part)
    most = mixer_product(
        me, blocks, (line, line_after, line_before), (0, 1, 3), None, length // 2
    )
    returned, most = lax.optimization_barrier((returned, most))
    returned_own = returned[:, 0].reshape(half, cols_part)
    returned_other = lax.ppermute(returned[:, 1].reshape(half, cols_part), "c", swap)
    mixed_out = mixer_product(
        me, blocks, (line_far_a, line_far_b), (2,), most, length
    )
    returned_other, mixed_out = lax.optimization_barrier((returned_other, mixed_out))
    expert_out = pl.pallas_call(
        functools.partial(combine_kernel, capacity=capacity),
        out_shape=jax.ShapeDtypeStruct((rows_b, cols_part), BF),
        compiler_params=pltpu.CompilerParams(vmem_limit_bytes=12 * 1024 * 1024),
    )(places, route_weights, returned_own, returned_other)
    return (mixed_out, expert_out)


def solution(mesh):
    ep, tp = mesh.devices.shape
    fine = Mesh(mesh.devices.reshape(ep // 2, 2, tp), ("z", "c", "tp"))
    both = ("z", "c")
    return jax.shard_map(
        layer,
        mesh=fine,
        in_specs=(
            P("tp", both),
            P("tp", both),
            P("tp", both),
            P(),
            P(None, "tp"),
            P(both, "tp"),
            P(both, None),
            P(both, None),
            P(both, None, "tp"),
            P(both, None, "tp"),
            P(both, "tp", None),
        ),
        out_specs=(P(both, "tp"), P(both, "tp")),
        check_vma=False,
    )
```
